32 devices in a mesh: grp: 2 (over x), fs: 4 (over z), tp: 4 (over y, core).
Axes of the slice: x: 2, y: 2, z: 4, core: 2. Of those that a mesh axis runs over, the one named last changes fastest.
Arguments:
- tokens: bfloat16 [1024, 3584], P(('grp', 'fs')), parts along dimension 0, may hold values from -6 to 6
- norm_gain: float32 [3584], P('fs'), may hold values from 0.1 to 1.9
- up_master: float32 [3584, 14336], P('fs', 'tp'), may hold values from -0.09375 to 0.09375
- down_master: float32 [3584, 14336], P('fs', 'tp'), may hold values from -0.046875 to 0.046875
Outputs:
- up_ready: bfloat16 [7168, 14336], P('grp', 'tp'), parts along dimension 0
- down_ready: bfloat16 [7168, 14336], P('grp', 'tp'), parts along dimension 0
- mixed_out: bfloat16 [1024, 3584], P(('grp', 'fs', 'tp')), parts along dimension 0
The draws below stay inside these ranges and needn't reach their ends.
There are 2 independent parts, one for each index of `grp`. The reference program is written for one: setup_inputs(seed, part) draws one part's arguments, and reference() takes and returns one part's arrays. A program takes and returns all parts, laid end to end along the dimension named above; an argument that names none is the same for every part. Nothing has to cross between parts.
All inputs are finite; a program needn't handle non-finite values.
Results may differ from the reference program's by a relative error of at most 0.024.
Values may be sent and summed in bfloat16 or wider, within the bound.
A program may use at most 192 MiB of HBM per device.

```python
import jax
import jax.numpy as jnp
from jax import lax

D = 3584
FF = 14336
TOKENS = 512


def steps_of(own_key, shape, pieces, low, top_value):
    loudness = 1.0
    for position, blocks in pieces:
        draws = jax.random.uniform(jax.random.fold_in(jax.random.fold_in(own_key, 6), position), (blocks,), jnp.float32, low / len(pieces), top_value / len(pieces))
        loudness = loudness * jnp.repeat(jnp.exp(draws), shape[position] // blocks).reshape((-1,) + (1,) * (len(shape) - 1 - position))
    return loudness


def noise(rng, shape, scale, most, pieces=(), held_as=jnp.bfloat16):
    loudness = steps_of(rng, shape, pieces, -0.22, 0.18) if pieces else 1.0
    values = jax.random.normal(rng, shape, jnp.float32) * scale * loudness
    return jnp.minimum(jnp.maximum(values, -most), most).astype(held_as)


def setup_inputs(seed: int = 0, part: int = 0) -> dict:
    keys = jax.random.split(jax.random.key(seed), 5)
    part_splits = jax.random.split(jax.random.fold_in(keys[4], part), 5)
    tokens = noise(part_splits[0], (TOKENS, D), 1.0, 6.0, ((0, 4),))
    norm_gain = jnp.clip(1.0 + 0.18 * jax.random.normal(keys[1], (D,), jnp.float32), 0.1, 1.9)
    up_master = noise(keys[2], (D, FF), D ** -0.5, 0.09375, ((0, 4), (1, 4)), jnp.float32)
    down_master = noise(keys[3], (D, FF), FF ** -0.5, 0.046875, ((0, 4), (1, 4)), jnp.float32)
    return dict(tokens=tokens, norm_gain=norm_gain, up_master=up_master, down_master=down_master)


def reference(tokens, norm_gain, up_master, down_master):
    up_ready = (norm_gain[:, None] * up_master).astype(jnp.bfloat16)
    down_ready = down_master.astype(jnp.bfloat16)
    values = tokens.astype(jnp.float32)
    square_mean = lax.optimization_barrier(jnp.mean(values * values, axis=1, keepdims=True))
    normed = (values * lax.rsqrt(square_mean + 1e-06)).astype(jnp.bfloat16)
    up_acts = jnp.dot(normed, up_ready, preferred_element_type=jnp.float32)
    hidden = jnp.square(jax.nn.relu(up_acts)).astype(jnp.bfloat16)
    mixed_out = lax.dot_general(hidden, down_ready, (((1,), (1,)), ((), ())), preferred_element_type=jnp.float32)
    return (up_ready, down_ready, mixed_out.astype(jnp.bfloat16))
```

```python
import functools

import jax
import jax.numpy as jnp
from jax import lax
from jax.experimental import pallas as pl
from jax.experimental.pallas import tpu as pltpu
from jax.sharding import PartitionSpec as P

MESH = pl.DeviceIdType.MESH
SLOTS = 12
LAG = 3


def divisor(total, most, least):
    for size in range(most, 0, -least):
        if total % size == 0:
            return size
    return total


def chunk_rows(block, width):
    for rows in range(16, block + 1, 16):
        if block % rows == 0 and rows * width * 2 >= 100 * 1024:
            return rows
    return block


def gather_kernel(sizes, tokens, gain, up, down, both, part, wide, column, held, normed, acc, hidden, load, token_s, zs, zr, xs, xr):
    n, local, block, rows, piece = sizes
    half = local // 2
    count = half // rows
    per_block = block // rows
    blocks = half // block
    last = n - 1
    span = last * count
    total = 2 * span
    slots = wide.shape[0]
    g, f, t = lax.axis_index("grp"), lax.axis_index("fs"), lax.axis_index("tp")
    other = 1 - g
    pieces = acc.shape[0]
    double = jnp.minimum(f, last - f)

    def start_load(m, which, q, index):
        first = pl.multiple_of(which * half + q * rows, 16)
        slot = lax.rem(index, slots)
        pltpu.make_async_copy((up, down)[m].at[pl.ds(first, rows)], wide.at[slot], load.at[slot]).start()

    def next_load(index):
        @pl.when(index < count)
        def _():
            start_load(0, g, index, index)

        for m in range(2):
            @pl.when((index >= count) & (index < 3 * count) & (lax.rem(index + count, 2) == m))
            def _(m=m):
                start_load(m, other, lax.div(index - count, 2), index)

        @pl.when((index >= 3 * count) & (index < 4 * count))
        def _():
            start_load(1, g, index - 3 * count, index)

    def where(m, source, which, q):
        first = pl.multiple_of(source * local + which * half + q * rows, 16)
        return both.at[m, pl.ds(first, rows)]

    def convert(m, which, q, index):
        slot = lax.rem(index, slots)
        pltpu.make_async_copy(up.at[pl.ds(0, rows)], wide.at[slot], load.at[slot]).wait()
        near = pl.multiple_of(which * half + q * rows, 16)
        first = pl.multiple_of(f * local + which * half + q * rows, 16)
        values = wide[slot]
        if m == 0:
            values = column[pl.ds(near, rows)] * values
        both[m, pl.ds(first, rows)] = values.astype(jnp.bfloat16)
        next_load(index + slots)

    has = (f < last, f > 0)

    def hop(way):
        return (g, f + 1 if way == 0 else f - 1, t)

    def origin(way, k):
        return f - k if way == 0 else f + k

    def reach(way, k):
        return (k <= f) if way == 0 else (k <= last - f)

    def z_at(way, m, k, q):
        return ((way * 2 + m) * last + k) * count + q

    def along(way, m, k, q):
        place = where(m, origin(way, k), g, q)
        return pltpu.make_async_remote_copy(
            place, place, zs.at[z_at(way, m, k, q)], zr.at[z_at(way, m, k, q)],
            device_id=hop(way), device_id_type=MESH)

    def arrival(way, m, k, q):
        place = where(m, origin(way, k), g, q)
        return pltpu.make_async_remote_copy(
            place, place, zs.at[0], zr.at[z_at(way, m, k - 1, q)],
            device_id=hop(way), device_id_type=MESH)

    def x_at(way, m, k, q):
        two = k <= double
        base = jnp.where(two, 2 * count * (k - 1), count * (k - 1 + double))
        return m * span + base + jnp.where(two, 2 * q + way, q)

    def x_of(i):
        m, j = lax.div(i, span), lax.rem(i, span)
        two = j < 2 * count * double
        single = jnp.maximum(j - 2 * count * double, 0)
        k = jnp.where(two, 1 + lax.div(j, 2 * count), 1 + double + lax.div(single, count))
        q = jnp.where(two, lax.div(lax.rem(j, 2 * count), 2), lax.rem(single, count))
        up_side = jnp.where(two, lax.rem(j, 2), jnp.where(f < last - f, 1, 0))
        source = f + (2 * up_side - 1) * k
        return m, source, q

    def across(m, source, which, q, i):
        place = where(m, source, which, q)
        return pltpu.make_async_remote_copy(
            place, place, xs.at[i], xr.at[i], device_id=(other, f, t), device_id_type=MESH)

    def send_own(m, q):
        for way in range(2):
            @pl.when(has[way])
            def _(way=way):
                along(way, m, 0, q).start()

    lax.fori_loop(0, slots, lambda i, c: (next_load(i), c)[1], 0)
    token_copy = pltpu.make_async_copy(tokens, held, token_s.at[0])
    token_copy.start()

    barrier = pltpu.get_barrier_semaphore()
    for way in range(2):
        @pl.when(has[way])
        def _(way=way):
            pl.semaphore_signal(barrier, inc=1, device_id=hop(way), device_id_type=MESH)
    pl.semaphore_signal(barrier, inc=1, device_id=(other, f, t), device_id_type=MESH)
    step_rows = divisor(local, 128, 8)
    eye = lax.broadcasted_iota(jnp.int32, (step_rows, step_rows), 0) == lax.broadcasted_iota(
        jnp.int32, (step_rows, step_rows), 1)
    for i in range(local // step_rows):
        line = gain[i:i + 1, :]
        column[i * step_rows:(i + 1) * step_rows, :] = jnp.sum(
            jnp.where(eye, line, 0.0), axis=1, keepdims=True)
    pl.semaphore_wait(barrier, 1 + jnp.minimum(f, 1) + jnp.minimum(last - f, 1))

    def first_step(q, carry):
        convert(0, g, q, q)

        @pl.when(q > 0)
        def _():
            send_own(0, q - 1)
        return carry

    lax.fori_loop(0, count, first_step, 0)
    token_copy.wait()
    values = held[...].astype(jnp.float32)
    square_mean = jnp.mean(values * values, axis=1, keepdims=True)
    send_own(0, count - 1)
    scaled = (values * lax.rsqrt(square_mean + 1e-06)).astype(jnp.bfloat16)
    for i in range(normed.shape[0]):
        normed[i] = scaled[:, i * block:(i + 1) * block]
    acc[...] = jnp.zeros_like(acc)

    def task(m, index):
        first = pl.multiple_of(index * block, 16)

        @pl.when(m == 0)
        def _():
            def body(p, carry):
                at = pl.multiple_of(p * piece, piece)
                acc[p] += jnp.dot(
                    normed[index], both[0, pl.ds(first, block), pl.ds(at, piece)],
                    preferred_element_type=jnp.float32)
                return carry
            lax.fori_loop(0, pieces, body, 0)

        @pl.when(m == 1)
        def _():
            def body(p, value):
                at = pl.multiple_of(p * piece, piece)
                return value + lax.dot_general(
                    hidden[p], both[1, pl.ds(first, block), pl.ds(at, piece)],
                    (((1,), (1,)), ((), ())), preferred_element_type=jnp.float32)
            value = lax.fori_loop(0, pieces, body, jnp.zeros((hidden.shape[1], block), jnp.float32))
            part[index] = value.astype(jnp.bfloat16)

    def forward(s):
        m, j = lax.div(s, span), lax.rem(s, span)
        k, q = 1 + lax.div(j, count), lax.rem(j, count)

        @pl.when(s < count)
        def _():
            for w in range(2):
                convert(w, other, s, count + 2 * s + w)

        @pl.when((s >= span - count) & (s < span))
        def _():
            convert(1, g, s - (span - count), 3 * count + s - (span - count))

        @pl.when((s > span - count) & (s <= span))
        def _():
            send_own(1, s - 1 - (span - count))

        for way in range(2):
            @pl.when(reach(way, k))
            def _(way=way):
                arrival(way, m, k, q).wait_recv()

                @pl.when(has[way])
                def _():
                    along(way, m, k, q).start()
                across(m, origin(way, k), g, q, x_at(way, m, k, q)).start()

    def absorb(i):
        m, j = lax.div(i, span), lax.rem(i, span)
        k, q = 1 + lax.div(j, count), lax.rem(j, count)
        _, source, xq = x_of(i)
        across(m, source, other, xq, i).wait_recv()
        every = 2 * blocks
        own = j - count

        def one(c, carry):
            z_full = lax.rem(q, per_block) == per_block - 1
            x_full = lax.rem(xq, per_block) == per_block - 1
            exists = jnp.where(
                c == 0, (k <= f) & z_full, jnp.where(
                    c == 1, (k <= last - f) & z_full, jnp.where(
                        c == 2, x_full, (own >= 0) & (own < every))))
            z_block = g * blocks + lax.div(q, per_block)
            index = jnp.where(
                c == 0, (f - k) * every + z_block, jnp.where(
                    c == 1, (f + k) * every + z_block, jnp.where(
                        c == 2, source * every + other * blocks + lax.div(xq, per_block),
                        f * every + own)))

            @pl.when(exists)
            def _():
                task(m, index)
            return carry

        lax.fori_loop(0, 4, one, 0)

        @pl.when(i == span - 1)
        def _():
            for p in range(pieces):
                hidden[p] = jnp.square(jnp.maximum(acc[p], 0.0)).astype(jnp.bfloat16)

    def step(s, carry):
        @pl.when(s < total)
        def _():
            forward(s)

        @pl.when(s >= LAG)
        def _():
            absorb(s - LAG)
        return carry

    lax.fori_loop(0, total + LAG, step, 0)

    def finish(s, carry):
        m, j = lax.div(s, span), lax.rem(s, span)
        k, q = lax.div(j, count), lax.rem(j, count)
        for way in range(2):
            @pl.when(has[way] & ((k == 0) | reach(way, k)))
            def _(way=way):
                along(way, m, k, q).wait_send()
        _, source, xq = x_of(s)
        across(m, source, g, xq, s).wait_send()
        return carry

    lax.fori_loop(0, total, finish, 0)


def gather(n, tokens, gain, up, down):
    local, width = up.shape
    count_rows = tokens.shape[0]
    half = local // 2
    block = divisor(half, 128, 16)
    rows = chunk_rows(block, width)
    count = half // rows
    depth = n * local
    piece = next(size for size in (512, 256, 128, width) if width % size == 0)
    moves = 2 * (n - 1) * count
    dma = pltpu.SemaphoreType.DMA
    step_rows = divisor(local, 128, 8)
    sent = 3 * (n - 1) * local * width * 2
    anywhere = pl.BlockSpec(memory_space=pl.ANY)
    inside = pl.BlockSpec(memory_space=pltpu.VMEM)
    return pl.pallas_call(
        functools.partial(gather_kernel, (n, local, block, rows, piece)),
        out_shape=[
            pltpu.VMEM((2, depth, width), jnp.bfloat16),
            pltpu.VMEM((depth // block, count_rows, block), jnp.bfloat16),
        ],
        in_specs=[anywhere, inside, anywhere, anywhere],
        out_specs=[inside, inside],
        scratch_shapes=[
            pltpu.VMEM((min(SLOTS, 4 * count), rows, width), jnp.float32),
            pltpu.VMEM((local, 1), jnp.float32),
            pltpu.VMEM((count_rows, depth), jnp.bfloat16),
            pltpu.VMEM((depth // block, count_rows, block), jnp.bfloat16),
            pltpu.VMEM((width // piece, count_rows, piece), jnp.float32),
            pltpu.VMEM((width // piece, count_rows, piece), jnp.bfloat16),
            dma((min(SLOTS, 4 * count),)),
            dma((1,)),
            dma((2 * moves,)),
            dma((2 * moves,)),
            dma((moves,)),
            dma((moves,)),
        ],
        compiler_params=pltpu.CompilerParams(
            collective_id=0, has_side_effects=True, vmem_limit_bytes=11 * 1024 * 1024),
        cost_estimate=pl.CostEstimate(flops=0, bytes_accessed=sent, transcendentals=0),
        name="gather_both",
    )(tokens, gain.reshape(local // step_rows, step_rows), up, down)


def sum_kernel(chips, part, out, pair, near, far, send, recv):
    g, f, t = lax.axis_index("grp"), lax.axis_index("fs"), lax.axis_index("tp")
    y, c = t // 2, lax.rem(t, 2)
    sibling = (g, f, 2 * y + 1 - c)

    def other(j):
        return lax.rem(y + j, chips)

    barrier = pltpu.get_barrier_semaphore()
    pl.semaphore_signal(barrier, inc=1, device_id=sibling, device_id_type=MESH)
    for j in range(1, chips):
        pl.semaphore_signal(barrier, inc=1, device_id=(g, f, 2 * other(j) + c), device_id_type=MESH)
    pl.semaphore_wait(barrier, chips)
    over, back = [], []
    for j in list(range(1, chips)) + [0]:
        copy = pltpu.make_async_remote_copy(
            part.at[2 * other(j) + 1 - c], near.at[j], send.at[j], recv.at[j],
            device_id=sibling, device_id_type=MESH)
        copy.start()
        over.append((j, copy))
    for j, copy in over:
        copy.wait_recv()
        both = part[2 * other(j) + c].astype(jnp.float32) + near[j].astype(jnp.float32)
        if j == 0:
            total = both
        else:
            pair[j] = both.astype(jnp.bfloat16)
            copy = pltpu.make_async_remote_copy(
                pair.at[j], far.at[j], send.at[chips + j], recv.at[chips + j],
                device_id=(g, f, 2 * other(j) + c), device_id_type=MESH)
            copy.start()
            back.append((j, copy))
    for j, copy in back:
        copy.wait_recv()
        total = total + far[j].astype(jnp.float32)
    out[...] = total.astype(jnp.bfloat16)
    for _, copy in over + back:
        copy.wait_send()


def write_kernel(parts, both, mixed, up_ready, down_ready, mixed_out, done):
    depth = both.shape[1]
    size = depth // parts
    copies = [pltpu.make_async_copy(mixed, mixed_out, done.at[2 * parts])]
    for m, ready in enumerate((up_ready, down_ready)):
        for i in range(parts):
            place = pl.ds(i * size, size)
            copies.append(pltpu.make_async_copy(both.at[m, place], ready.at[place], done.at[m * parts + i]))
    for copy in copies:
        copy.start()
    for copy in copies:
        copy.wait()


def per_device(n, tp, tokens, norm_gain, up_master, down_master):
    both, part = gather(n, tokens, norm_gain, up_master, down_master)
    depth, width = both.shape[1:]
    count = tokens.shape[0]
    mixed = part.transpose(1, 0, 2).reshape(count, depth)
    share = count // tp
    chips = tp // 2
    held = pltpu.VMEM((chips, share, depth), jnp.bfloat16)
    mixed_sum = pl.pallas_call(
        functools.partial(sum_kernel, chips),
        out_shape=jax.ShapeDtypeStruct((share, depth), jnp.bfloat16),
        in_specs=[pl.BlockSpec(memory_space=pltpu.VMEM)],
        out_specs=pl.BlockSpec(memory_space=pltpu.VMEM),
        scratch_shapes=[held, held, held] + [pltpu.SemaphoreType.DMA((2 * chips,))] * 2,
        compiler_params=pltpu.CompilerParams(
            collective_id=1, has_side_effects=True, vmem_limit_bytes=8 * 1024 * 1024),
        name="sum_shares",
    )(mixed.reshape(tp, share, depth))
    weight = jax.ShapeDtypeStruct((depth, width), jnp.bfloat16)
    anywhere = pl.BlockSpec(memory_space=pl.ANY)
    parts = 8
    return tuple(pl.pallas_call(
        functools.partial(write_kernel, parts),
        out_shape=[weight, weight, jax.ShapeDtypeStruct((share, depth), jnp.bfloat16)],
        in_specs=[anywhere, anywhere],
        out_specs=[anywhere] * 3,
        scratch_shapes=[pltpu.SemaphoreType.DMA((2 * parts + 1,))],
        compiler_params=pltpu.CompilerParams(vmem_limit_bytes=1024 * 1024),
        name="write_out",
    )(both, mixed_sum))


def solution(mesh):
    n, tp = (mesh.shape[name] for name in ("fs", "tp"))
    return jax.shard_map(
        functools.partial(per_device, n, tp),
        mesh=mesh,
        in_specs=(P(("grp", "fs"), None), P("fs"), P("fs", "tp"), P("fs", "tp")),
        out_specs=(P("grp", "tp"), P("grp", "tp"), P(("grp", "fs", "tp"), None)),
        check_vma=False,
    )
```

```python
import functools

import jax
import jax.numpy as jnp
from jax import lax
from jax.experimental import pallas as pl
from jax.experimental.pallas import tpu as pltpu
from jax.sharding import PartitionSpec as P

MESH = pl.DeviceIdType.MESH
SLOTS = 12
LAG = 5


def divisor(total, most, least):
    for size in range(most, 0, -least):
        if total % size == 0:
            return size
    return total


def chunk_rows(block, width):
    for rows in range(16, block + 1, 16):
        if block % rows == 0 and rows * width * 2 >= 100 * 1024:
            return rows
    return block


def gather_kernel(sizes, tokens, gain, up, down, both, out, wide, column, held, normed, acc, hidden, product,
                  part, near, pair, kept, far, load, token_s, zs, zr, xs, xr, ss, sr, bs, br):
    n, tp, local, block, rows, piece = sizes
    half = local // 2
    count = half // rows
    per_block = block // rows
    blocks = half // block
    last = n - 1
    span = last * count
    total = 2 * span
    slots = wide.shape[0]
    g, f, t = lax.axis_index("grp"), lax.axis_index("fs"), lax.axis_index("tp")
    other = 1 - g
    chips = tp // 2
    y, c = t // 2, lax.rem(t, 2)
    every = 2 * blocks
    share = kept.shape[1]
    pieces = acc.shape[0]
    each = -(-pieces // per_block)
    double = jnp.minimum(f, last - f)

    def start_load(m, which, q, index):
        first = pl.multiple_of(which * half + q * rows, 16)
        slot = lax.rem(index, slots)
        pltpu.make_async_copy((up, down)[m].at[pl.ds(first, rows)], wide.at[slot], load.at[slot]).start()

    def next_load(index):
        @pl.when(index < count)
        def _():
            start_load(0, g, index, index)

        for m in range(2):
            @pl.when((index >= count) & (index < 3 * count) & (lax.rem(index + count, 2) == m))
            def _(m=m):
                start_load(m, other, lax.div(index - count, 2), index)

        @pl.when((index >= 3 * count) & (index < 4 * count))
        def _():
            start_load(1, g, index - 3 * count, index)

    def where(m, source, which, q):
        first = pl.multiple_of(source * local + which * half + q * rows, 16)
        return both.at[m, pl.ds(first, rows)]

    def convert(m, which, q, index):
        slot = lax.rem(index, slots)
        pltpu.make_async_copy(up.at[pl.ds(0, rows)], wide.at[slot], load.at[slot]).wait()
        near = pl.multiple_of(which * half + q * rows, 16)
        first = pl.multiple_of(f * local + which * half + q * rows, 16)
        values = wide[slot]
        if m == 0:
            values = column[pl.ds(near, rows)] * values
        both[m, pl.ds(first, rows)] = values.astype(jnp.bfloat16)
        next_load(index + slots)

    has = (f < last, f > 0)

    def hop(way):
        return (g, f + 1 if way == 0 else f - 1, t)

    def origin(way, k):
        return f - k if way == 0 else f + k

    def reach(way, k):
        return (k <= f) if way == 0 else (k <= last - f)

    def z_at(way, m, k, q):
        return ((way * 2 + m) * last + k) * count + q

    def along(way, m, k, q):
        place = where(m, origin(way, k), g, q)
        return pltpu.make_async_remote_copy(
            place, place, zs.at[z_at(way, m, k, q)], zr.at[z_at(way, m, k, q)],
            device_id=hop(way), device_id_type=MESH)

    def arrival(way, m, k, q):
        place = where(m, origin(way, k), g, q)
        return pltpu.make_async_remote_copy(
            place, place, zs.at[0], zr.at[z_at(way, m, k - 1, q)],
            device_id=hop(way), device_id_type=MESH)

    def x_at(way, m, k, q):
        two = k <= double
        base = jnp.where(two, 2 * count * (k - 1), count * (k - 1 + double))
        return m * span + base + jnp.where(two, 2 * q + way, q)

    def x_of(i):
        m, j = lax.div(i, span), lax.rem(i, span)
        two = j < 2 * count * double
        single = jnp.maximum(j - 2 * count * double, 0)
        k = jnp.where(two, 1 + lax.div(j, 2 * count), 1 + double + lax.div(single, count))
        q = jnp.where(two, lax.div(lax.rem(j, 2 * count), 2), lax.rem(single, count))
        up_side = jnp.where(two, lax.rem(j, 2), jnp.where(f < last - f, 1, 0))
        source = f + (2 * up_side - 1) * k
        return m, source, q

    def across(m, source, which, q, i):
        place = where(m, source, which, q)
        return pltpu.make_async_remote_copy(
            place, place, xs.at[i], xr.at[i], device_id=(other, f, t), device_id_type=MESH)

    def send_own(m, q):
        for way in range(2):
            @pl.when(has[way])
            def _(way=way):
                along(way, m, 0, q).start()

    lax.fori_loop(0, slots, lambda i, c: (next_load(i), c)[1], 0)
    token_copy = pltpu.make_async_copy(tokens, held, token_s.at[0])
    token_copy.start()

    barrier = pltpu.get_barrier_semaphore()
    for way in range(2):
        @pl.when(has[way])
        def _(way=way):
            pl.semaphore_signal(barrier, inc=1, device_id=hop(way), device_id_type=MESH)
    pl.semaphore_signal(barrier, inc=1, device_id=(other, f, t), device_id_type=MESH)
    sibling = (g, f, 2 * y + 1 - c)
    pl.semaphore_signal(barrier, inc=1, device_id=sibling, device_id_type=MESH)

    def chip(j):
        return lax.rem(y + j, chips)

    for j in range(1, chips):
        pl.semaphore_signal(barrier, inc=1, device_id=(g, f, 2 * chip(j) + c), device_id_type=MESH)
    step_rows = divisor(local, 128, 8)
    eye = lax.broadcasted_iota(jnp.int32, (step_rows, step_rows), 0) == lax.broadcasted_iota(
        jnp.int32, (step_rows, step_rows), 1)
    for i in range(local // step_rows):
        line = gain[i:i + 1, :]
        column[i * step_rows:(i + 1) * step_rows, :] = jnp.sum(
            jnp.where(eye, line, 0.0), axis=1, keepdims=True)
    pl.semaphore_wait(barrier, 1 + chips + jnp.minimum(f, 1) + jnp.minimum(last - f, 1))

    def first_step(q, carry):
        convert(0, g, q, q)

        @pl.when(q > 0)
        def _():
            send_own(0, q - 1)
        return carry

    lax.fori_loop(0, count, first_step, 0)
    token_copy.wait()
    values = held[...].astype(jnp.float32)
    square_mean = jnp.mean(values * values, axis=1, keepdims=True)
    send_own(0, count - 1)
    scaled = (values * lax.rsqrt(square_mean + 1e-06)).astype(jnp.bfloat16)
    scaled = jnp.concatenate(
        [scaled[i * share:(i + 1) * share] for i in list(range(0, tp, 2)) + list(range(1, tp, 2))])
    for i in range(normed.shape[0]):
        normed[i] = scaled[:, i * block:(i + 1) * block]
    acc[...] = jnp.zeros_like(acc)

    def slot_of(period, slot):
        i = period * per_block - 1
        m, j = lax.div(i, span), lax.rem(i, span)
        k, q = 1 + lax.div(j, count), lax.rem(j, count)
        z_block = g * blocks + lax.div(q, per_block)
        two = j < 2 * count * double
        single = jnp.maximum(j - 2 * count * double, 0)
        xk = jnp.where(two, 1 + lax.div(j, 2 * count), 1 + double + lax.div(single, count))
        xq = jnp.where(two, lax.div(lax.rem(j, 2 * count), 2), lax.rem(single, count))
        x_full = jnp.where(two, lax.rem(j, 2 * per_block) == 2 * per_block - 1, slot == 2)
        above = jnp.where(two, slot == 3, f < last - f)
        source = jnp.where(above, f + xk, f - xk)
        own = lax.div(j - count, per_block)
        exists = (period > 0) & jnp.where(
            slot == 0, k <= f, jnp.where(
                slot == 1, k <= last - f, jnp.where(
                    slot == 4, (j >= count) & (own < every), x_full)))
        index = jnp.where(
            slot == 0, (f - k) * every + z_block, jnp.where(
                slot == 1, (f + k) * every + z_block, jnp.where(
                    slot == 4, f * every + own,
                    source * every + other * blocks + lax.div(xq, per_block))))
        return exists, m, index

    def multiply(m, index, slot, p):
        first = pl.multiple_of(index * block, 16)
        at = pl.multiple_of(p * piece, piece)

        @pl.when(m == 0)
        def _():
            acc[p] += jnp.dot(
                normed[index], both[0, pl.ds(first, block), pl.ds(at, piece)],
                preferred_element_type=jnp.float32)

        @pl.when(m == 1)
        def _():
            value = lax.dot_general(
                hidden[p], both[1, pl.ds(first, block), pl.ds(at, piece)],
                (((1,), (1,)), ((), ())), preferred_element_type=jnp.float32)

            @pl.when(p == 0)
            def _():
                product[slot] = value

            @pl.when(p > 0)
            def _():
                product[slot] += value

    mine = pl.multiple_of(c * (chips * share), 4)
    theirs = pl.multiple_of((1 - c) * (chips * share), 4)

    def over(index):
        return pltpu.make_async_remote_copy(
            part.at[index, pl.ds(theirs, chips * share)], near.at[index], ss.at[index], sr.at[index],
            device_id=sibling, device_id_type=MESH)

    def back(index, j):
        at = index * (chips - 1) + j - 1
        return pltpu.make_async_remote_copy(
            pair.at[index, chip(j)], far.at[index, j - 1], bs.at[at], br.at[at],
            device_id=(g, f, 2 * chip(j) + c), device_id_type=MESH)

    def stage(which, period):
        def one(slot, carry):
            exists, m, index = slot_of(period, slot)

            @pl.when(exists & (m == 1))
            def _():
                if which == 0:
                    part[index] = product[slot].astype(jnp.bfloat16)
                elif which == 1:
                    over(index).start()
                elif which == 2:
                    over(index).wait_recv()
                    value = part[index, pl.ds(mine, chips * share)].astype(jnp.float32) + near[index].astype(jnp.float32)
                    for j in range(chips):
                        rows_j = value[j * share:(j + 1) * share]
                        pair[index, j] = rows_j.astype(jnp.bfloat16)

                        @pl.when(y == j)
                        def _(rows_j=rows_j):
                            kept[index] = rows_j
                elif which == 3:
                    for j in range(1, chips):
                        back(index, j).start()
                else:
                    value = kept[index]
                    for j in range(1, chips):
                        back(index, j).wait_recv()
                        value = value + far[index, j - 1].astype(jnp.float32)
                    out[index] = value.astype(jnp.bfloat16)
            return carry

        lax.fori_loop(0, 5, one, 0)

    def forward(s):
        m, j = lax.div(s, span), lax.rem(s, span)
        k, q = 1 + lax.div(j, count), lax.rem(j, count)

        @pl.when(s < count)
        def _():
            for w in range(2):
                convert(w, other, s, count + 2 * s + w)

        @pl.when((s >= span - count) & (s < span))
        def _():
            convert(1, g, s - (span - count), 3 * count + s - (span - count))

        @pl.when((s > span - count) & (s <= span))
        def _():
            send_own(1, s - 1 - (span - count))

        for way in range(2):
            @pl.when(reach(way, k))
            def _(way=way):
                arrival(way, m, k, q).wait_recv()

                @pl.when(has[way])
                def _():
                    along(way, m, k, q).start()
                across(m, origin(way, k), g, q, x_at(way, m, k, q)).start()

    def absorb(i):
        @pl.when(i < total)
        def _():
            _, source, xq = x_of(i)
            across(0, source, other, xq, i).wait_recv()

        period, p = lax.div(i, per_block), lax.rem(i, per_block)

        def one(slot, carry):
            exists, m, index = slot_of(period, slot)

            @pl.when(exists)
            def _():
                def body(r, carry):
                    multiply(m, index, slot, r)
                    return carry
                lax.fori_loop(p * each, jnp.minimum((p + 1) * each, pieces), body, 0)
            return carry

        lax.fori_loop(0, 5, one, 0)

        @pl.when(p == per_block - 1)
        def _():
            stage(0, period)
            stage(2, period - 1)
            stage(1, period)
            stage(3, period - 1)
            stage(4, period - 2)

        @pl.when(i == span + per_block - 1)
        def _():
            for r in range(pieces):
                hidden[r] = jnp.square(jnp.maximum(acc[r], 0.0)).astype(jnp.bfloat16)

    def step(s, carry):
        @pl.when(s < total)
        def _():
            forward(s)

        @pl.when(s >= LAG)
        def _():
            absorb(s - LAG)
        return carry

    lax.fori_loop(0, total + LAG + per_block, step, 0)
    final = total // per_block
    stage(2, final)
    stage(3, final)
    stage(4, final - 1)
    stage(4, final)

    def finish(s, carry):
        m, j = lax.div(s, span), lax.rem(s, span)
        k, q = lax.div(j, count), lax.rem(j, count)
        for way in range(2):
            @pl.when(has[way] & ((k == 0) | reach(way, k)))
            def _(way=way):
                along(way, m, k, q).wait_send()
        _, source, xq = x_of(s)
        across(m, source, g, xq, s).wait_send()
        return carry

    lax.fori_loop(0, total, finish, 0)

    def finish_sum(index, carry):
        over(index).wait_send()
        for j in range(1, chips):
            back(index, j).wait_send()
        return carry

    lax.fori_loop(0, n * every, finish_sum, 0)


def gather(n, tp, tokens, gain, up, down):
    local, width = up.shape
    count_rows = tokens.shape[0]
    half = local // 2
    block = divisor(half, 128, 16)
    rows = chunk_rows(block, width)
    count = half // rows
    depth = n * local
    piece = next(size for size in (512, 256, 128, width) if width % size == 0)
    moves = 2 * (n - 1) * count
    share, chips, total = count_rows // tp, tp // 2, depth // block
    dma = pltpu.SemaphoreType.DMA
    step_rows = divisor(local, 128, 8)
    sent = 3 * (n - 1) * local * width * 2
    anywhere = pl.BlockSpec(memory_space=pl.ANY)
    inside = pl.BlockSpec(memory_space=pltpu.VMEM)
    return pl.pallas_call(
        functools.partial(gather_kernel, (n, tp, local, block, rows, piece)),
        out_shape=[
            pltpu.VMEM((2, depth, width), jnp.bfloat16),
            pltpu.VMEM((total, share, block), jnp.bfloat16),
        ],
        in_specs=[anywhere, inside, anywhere, anywhere],
        out_specs=[inside, inside],
        scratch_shapes=[
            pltpu.VMEM((min(SLOTS, 4 * count), rows, width), jnp.float32),
            pltpu.VMEM((local, 1), jnp.float32),
            pltpu.VMEM((count_rows, depth), jnp.bfloat16),
            pltpu.VMEM((depth // block, count_rows, block), jnp.bfloat16),
            pltpu.VMEM((width // piece, count_rows, piece), jnp.float32),
            pltpu.VMEM((width // piece, count_rows, piece), jnp.bfloat16),
            pltpu.VMEM((5, count_rows, block), jnp.float32),
            pltpu.VMEM((total, count_rows, block), jnp.bfloat16),
            pltpu.VMEM((total, count_rows // 2, block), jnp.bfloat16),
            pltpu.VMEM((total, chips, share, block), jnp.bfloat16),
            pltpu.VMEM((total, share, block), jnp.float32),
            pltpu.VMEM((total, chips - 1, share, block), jnp.bfloat16),
            dma((min(SLOTS, 4 * count),)),
            dma((1,)),
            dma((2 * moves,)),
            dma((2 * moves,)),
            dma((moves,)),
            dma((moves,)),
            dma((total,)),
            dma((total,)),
            dma((total * (chips - 1),)),
            dma((total * (chips - 1),)),
        ],
        compiler_params=pltpu.CompilerParams(
            collective_id=0, has_side_effects=True, vmem_limit_bytes=27 * 512 * 1024),
        cost_estimate=pl.CostEstimate(flops=0, bytes_accessed=sent, transcendentals=0),
        name="gather_both",
    )(tokens, gain.reshape(local // step_rows, step_rows), up, down)


def write_kernel(parts, both, mixed, up_ready, down_ready, mixed_out, done):
    depth = both.shape[1]
    size = depth // parts
    copies = []
    for m, ready in enumerate((up_ready, down_ready)):
        for i in range(parts):
            place = pl.ds(i * size, size)
            copies.append(pltpu.make_async_copy(both.at[m, place], ready.at[place], done.at[m * parts + i]))
    for copy in copies:
        copy.start()
    block = mixed.shape[2]
    for i in range(mixed.shape[0]):
        mixed_out[:, i * block:(i + 1) * block] = mixed[i]
    for copy in copies:
        copy.wait()


def per_device(n, tp, tokens, norm_gain, up_master, down_master):
    both, mixed = gather(n, tp, tokens, norm_gain, up_master, down_master)
    depth, width = both.shape[1:]
    share = mixed.shape[1]
    weight = jax.ShapeDtypeStruct((depth, width), jnp.bfloat16)
    anywhere = pl.BlockSpec(memory_space=pl.ANY)
    inside = pl.BlockSpec(memory_space=pltpu.VMEM)
    parts = 8
    return tuple(pl.pallas_call(
        functools.partial(write_kernel, parts),
        out_shape=[weight, weight, jax.ShapeDtypeStruct((share, depth), jnp.bfloat16)],
        in_specs=[anywhere, inside],
        out_specs=[anywhere, anywhere, inside],
        scratch_shapes=[pltpu.SemaphoreType.DMA((2 * parts,))],
        compiler_params=pltpu.CompilerParams(vmem_limit_bytes=27 * 512 * 1024),
        name="write_out",
    )(pltpu.with_memory_space_constraint(both, pltpu.VMEM), pltpu.with_memory_space_constraint(mixed, pltpu.VMEM)))


def solution(mesh):
    n, tp = (mesh.shape[name] for name in ("fs", "tp"))
    return jax.shard_map(
        functools.partial(per_device, n, tp),
        mesh=mesh,
        in_specs=(P(("grp", "fs"), None), P("fs"), P("fs", "tp"), P("fs", "tp")),
        out_specs=(P("grp", "tp"), P("grp", "tp"), P(("grp", "fs", "tp"), None)),
        check_vma=False,
    )
```

```python
import functools

import jax
import jax.numpy as jnp
from jax import lax
from jax.experimental import pallas as pl
from jax.experimental.pallas import tpu as pltpu
from jax.sharding import PartitionSpec as P

MESH = pl.DeviceIdType.MESH
SLOTS = 6
LAG = 2


def divisor(total, most, least):
    for size in range(most, 0, -least):
        if total % size == 0:
            return size
    return total


def chunk_rows(block, width):
    for rows in range(16, block + 1, 16):
        if block % rows == 0 and rows * width * 2 >= 200 * 1024:
            return rows
    return block


def gather_kernel(sizes, tokens, gain, up, down, both, out, wide, column, held, normed, acc, hidden, product,
                  part, near, pair, kept, far, load, token_s, zs, zr, xs, xr, ss, sr, bs, br):
    n, tp, local, block, rows, piece = sizes
    half = local // 2
    count = half // rows
    per_block = block // rows
    blocks = half // block
    last = n - 1
    span = last * count
    total = 2 * span
    slots = wide.shape[0]
    g, f, t = lax.axis_index("grp"), lax.axis_index("fs"), lax.axis_index("tp")
    other = 1 - g
    chips = tp // 2
    y, c = t // 2, lax.rem(t, 2)
    every = 2 * blocks
    share = kept.shape[1]
    pieces = acc.shape[0]
    each = -(-pieces // per_block)
    double = jnp.minimum(f, last - f)

    def start_load(m, which, q, index):
        first = pl.multiple_of(which * half + q * rows, 16)
        slot = lax.rem(index, slots)
        pltpu.make_async_copy((up, down)[m].at[pl.ds(first, rows)], wide.at[slot], load.at[slot]).start()

    def next_load(index):
        @pl.when(index < count)
        def _():
            start_load(0, g, index, index)

        for m in range(2):
            @pl.when((index >= count) & (index < 3 * count) & (lax.rem(index + count, 2) == m))
            def _(m=m):
                start_load(m, other, lax.div(index - count, 2), index)

        @pl.when((index >= 3 * count) & (index < 4 * count))
        def _():
            start_load(1, g, index - 3 * count, index)

    def where(m, source, which, q):
        first = pl.multiple_of(source * local + which * half + q * rows, 16)
        return both.at[m, pl.ds(first, rows)]

    def convert(m, which, q, index):
        slot = lax.rem(index, slots)
        pltpu.make_async_copy(up.at[pl.ds(0, rows)], wide.at[slot], load.at[slot]).wait()
        near = pl.multiple_of(which * half + q * rows, 16)
        first = pl.multiple_of(f * local + which * half + q * rows, 16)
        values = wide[slot]
        if m == 0:
            values = column[pl.ds(near, rows)] * values
        both[m, pl.ds(first, rows)] = values.astype(jnp.bfloat16)
        next_load(index + slots)

    has = (f < last, f > 0)

    def hop(way):
        return (g, f + 1 if way == 0 else f - 1, t)

    def origin(way, k):
        return f - k if way == 0 else f + k

    def reach(way, k):
        return (k <= f) if way == 0 else (k <= last - f)

    def z_at(way, m, k, q):
        return ((way * 2 + m) * last + k) * count + q

    def along(way, m, k, q):
        place = where(m, origin(way, k), g, q)
        return pltpu.make_async_remote_copy(
            place, place, zs.at[(way * 2 + m) * last + k], zr.at[z_at(way, m, k, q)],
            device_id=hop(way), device_id_type=MESH)

    def all_rows(m, source, way, k, across_x):
        place = both.at[m, pl.ds(pl.multiple_of(source * local + g * half, 16), half)]
        at = (way * 2 + m) * last + k
        return pltpu.make_async_remote_copy(
            place, place, (xs if across_x else zs).at[at], zr.at[0],
            device_id=(other, f, t) if across_x else hop(way), device_id_type=MESH)

    def arrival(way, m, k, q):
        place = where(m, origin(way, k), g, q)
        return pltpu.make_async_remote_copy(
            place, place, zs.at[0], zr.at[z_at(way, m, k - 1, q)],
            device_id=hop(way), device_id_type=MESH)

    def x_at(way, m, k, q):
        two = k <= double
        base = jnp.where(two, 2 * count * (k - 1), count * (k - 1 + double))
        return m * span + base + jnp.where(two, 2 * q + way, q)

    def x_of(i):
        m, j = lax.div(i, span), lax.rem(i, span)
        two = j < 2 * count * double
        single = jnp.maximum(j - 2 * count * double, 0)
        k = jnp.where(two, 1 + lax.div(j, 2 * count), 1 + double + lax.div(single, count))
        q = jnp.where(two, lax.div(lax.rem(j, 2 * count), 2), lax.rem(single, count))
        up_side = jnp.where(two, lax.rem(j, 2), jnp.where(f < last - f, 1, 0))
        source = f + (2 * up_side - 1) * k
        return m, source, q

    def across(m, source, which, q, sent, i):
        place = where(m, source, which, q)
        return pltpu.make_async_remote_copy(
            place, place, xs.at[sent], xr.at[i], device_id=(other, f, t), device_id_type=MESH)

    def send_own(m, q):
        for way in range(2):
            @pl.when(has[way])
            def _(way=way):
                along(way, m, 0, q).start()

    lax.fori_loop(0, slots, lambda i, c: (next_load(i), c)[1], 0)
    token_copy = pltpu.make_async_copy(tokens, held, token_s.at[0])
    token_copy.start()

    barrier = pltpu.get_barrier_semaphore()
    for way in range(2):
        @pl.when(has[way])
        def _(way=way):
            pl.semaphore_signal(barrier, inc=1, device_id=hop(way), device_id_type=MESH)
    pl.semaphore_signal(barrier, inc=1, device_id=(other, f, t), device_id_type=MESH)
    sibling = (g, f, 2 * y + 1 - c)
    pl.semaphore_signal(barrier, inc=1, device_id=sibling, device_id_type=MESH)

    def chip(j):
        return lax.rem(y + j, chips)

    for j in range(1, chips):
        pl.semaphore_signal(barrier, inc=1, device_id=(g, f, 2 * chip(j) + c), device_id_type=MESH)
    step_rows = divisor(local, 128, 8)
    eye = lax.broadcasted_iota(jnp.int32, (step_rows, step_rows), 0) == lax.broadcasted_iota(
        jnp.int32, (step_rows, step_rows), 1)
    for i in range(local // step_rows):
        line = gain[i:i + 1, :]
        column[i * step_rows:(i + 1) * step_rows, :] = jnp.sum(
            jnp.where(eye, line, 0.0), axis=1, keepdims=True)
    pl.semaphore_wait(barrier, 1 + chips + jnp.minimum(f, 1) + jnp.minimum(last - f, 1))

    def first_step(q, carry):
        convert(0, g, q, q)

        @pl.when(q > 0)
        def _():
            send_own(0, q - 1)
        return carry

    lax.fori_loop(0, count, first_step, 0)
    token_copy.wait()
    values = held[...].astype(jnp.float32)
    square_mean = jnp.mean(values * values, axis=1, keepdims=True)
    send_own(0, count - 1)
    scaled = (values * lax.rsqrt(square_mean + 1e-06)).astype(jnp.bfloat16)
    scaled = jnp.concatenate(
        [scaled[i * share:(i + 1) * share] for i in list(range(0, tp, 2)) + list(range(1, tp, 2))])
    for i in range(normed.shape[0]):
        normed[i] = scaled[:, i * block:(i + 1) * block]
    acc[...] = jnp.zeros_like(acc)

    def slot_of(period, slot):
        i = period * per_block - 1
        m, j = lax.div(i, span), lax.rem(i, span)
        k, q = 1 + lax.div(j, count), lax.rem(j, count)
        z_block = g * blocks + lax.div(q, per_block)
        two = j < 2 * count * double
        single = jnp.maximum(j - 2 * count * double, 0)
        xk = jnp.where(two, 1 + lax.div(j, 2 * count), 1 + double + lax.div(single, count))
        xq = jnp.where(two, lax.div(lax.rem(j, 2 * count), 2), lax.rem(single, count))
        x_full = jnp.where(two, lax.rem(j, 2 * per_block) == 2 * per_block - 1, slot == 2)
        above = jnp.where(two, slot == 3, f < last - f)
        source = jnp.where(above, f + xk, f - xk)
        own = lax.div(j + 1 - count, per_block)
        exists = (period > 0) & jnp.where(
            slot == 0, k <= f, jnp.where(
                slot == 1, k <= last - f, jnp.where(
                    slot == 4, (j + 1 >= count) & (own < every), x_full)))
        index = jnp.where(
            slot == 0, (f - k) * every + z_block, jnp.where(
                slot == 1, (f + k) * every + z_block, jnp.where(
                    slot == 4, f * every + own,
                    source * every + other * blocks + lax.div(xq, per_block))))
        return exists, m, index

    def multiply(m, index, slot, p):
        first = pl.multiple_of(index * block, 16)
        at = pl.multiple_of(p * piece, piece)

        @pl.when(m == 0)
        def _():
            acc[p] += jnp.dot(
                normed[index], both[0, pl.ds(first, block), pl.ds(at, piece)],
                preferred_element_type=jnp.float32)

        @pl.when(m == 1)
        def _():
            value = lax.dot_general(
                hidden[p], both[1, pl.ds(first, block), pl.ds(at, piece)],
                (((1,), (1,)), ((), ())), preferred_element_type=jnp.float32)

            @pl.when(p == 0)
            def _():
                product[slot] = value

            @pl.when(p > 0)
            def _():
                product[slot] += value

    mine = pl.multiple_of(c * (chips * share), 4)
    theirs = pl.multiple_of((1 - c) * (chips * share), 4)

    def over(index):
        return pltpu.make_async_remote_copy(
            part.at[index, pl.ds(theirs, chips * share)], near.at[index], ss.at[0], sr.at[index],
            device_id=sibling, device_id_type=MESH)

    def back(index, j):
        at = index * (chips - 1) + j - 1
        return pltpu.make_async_remote_copy(
            pair.at[index, chip(j)], far.at[index, j - 1], bs.at[j - 1], br.at[at],
            device_id=(g, f, 2 * chip(j) + c), device_id_type=MESH)

    def stage(which, period, low=0, high=5):
        def one(slot, carry):
            exists, m, index = slot_of(period, slot)

            @pl.when(exists & (m == 1))
            def _():
                if which == 0:
                    part[index] = product[slot].astype(jnp.bfloat16)
                elif which == 1:
                    over(index).start()
                elif which == 2:
                    over(index).wait_recv()
                    value = part[index, pl.ds(mine, chips * share)].astype(jnp.float32) + near[index].astype(jnp.float32)
                    for j in range(chips):
                        rows_j = value[j * share:(j + 1) * share]
                        pair[index, j] = rows_j.astype(jnp.bfloat16)

                        @pl.when(y == j)
                        def _(rows_j=rows_j):
                            kept[index] = rows_j
                elif which == 3:
                    for j in range(1, chips):
                        back(index, j).start()
                else:
                    value = kept[index]
                    for j in range(1, chips):
                        back(index, j).wait_recv()
                        value = value + far[index, j - 1].astype(jnp.float32)
                    out[index] = value.astype(jnp.bfloat16)
            return carry

        lax.fori_loop(low, high, one, 0)

    def forward(s):
        m, j = lax.div(s, span), lax.rem(s, span)
        k, q = 1 + lax.div(j, count), lax.rem(j, count)

        @pl.when(s < count)
        def _():
            for w in range(2):
                convert(w, other, s, count + 2 * s + w)

        @pl.when((s >= span - count) & (s < span))
        def _():
            convert(1, g, s - (span - count), 3 * count + s - (span - count))

        @pl.when((s > span - count) & (s <= span))
        def _():
            send_own(1, s - 1 - (span - count))

        for way in range(2):
            @pl.when(reach(way, k))
            def _(way=way):
                arrival(way, m, k, q).wait_recv()

                @pl.when(has[way])
                def _():
                    along(way, m, k, q).start()
                across(
                    m, origin(way, k), g, q, (way * 2 + m) * last + k - 1, x_at(way, m, k, q)).start()

    def run(period, low, high, first, end):
        def one(slot, carry):
            exists, m, index = slot_of(period, slot)

            @pl.when(exists)
            def _():
                def body(r, carry):
                    multiply(m, index, slot, r)
                    return carry
                lax.fori_loop(first, end, body, 0)
            return carry

        lax.fori_loop(low, high, one, 0)

    def absorb(i, low, high, wait):
        if wait:
            _, source, xq = x_of(i)
            across(0, source, other, xq, 0, i).wait_recv()
        period, p = lax.div(i, per_block), lax.rem(i, per_block)
        run(period, low, high, jnp.minimum(p * each, pieces), jnp.minimum((p + 1) * each, pieces))

        @pl.when(p == per_block - 1)
        def _():
            stage(0, period, low, high)
            if wait:
                stage(2, period - 1)
            stage(1, period, low, high)
            if wait:
                stage(3, period - 1)
                stage(4, period - 2)

        if wait:
            @pl.when(i == span + per_block - 1)
            def _():
                for r in range(pieces):
                    hidden[r] = jnp.square(jnp.maximum(acc[r], 0.0)).astype(jnp.bfloat16)

    def step(s, carry):
        forward(s)

        @pl.when(s >= LAG)
        def _():
            absorb(s - LAG, 0, 5, True)
        return carry

    lax.fori_loop(0, total, step, 0)
    final = total // per_block

    def drain(low, high, wait):
        def one(i, carry):
            absorb(i, low, high, wait)
            return carry

        lax.fori_loop(total - LAG, total, one, 0)
        run(final, low, high, 0, pieces)
        stage(0, final, low, high)
        stage(1, final, low, high)

    drain(0, 2, False)
    drain(2, 5, True)
    stage(2, final - 1)
    stage(3, final - 1)
    stage(2, final)
    stage(3, final)
    stage(4, final - 2)
    stage(4, final - 1)
    stage(4, final)

    def finish(r, carry):
        m, k = lax.div(r, last), lax.rem(r, last)
        for way in range(2):
            @pl.when(has[way] & ((k == 0) | reach(way, k)))
            def _(way=way):
                all_rows(m, origin(way, k), way, k, False).wait_send()

            @pl.when(reach(way, k + 1))
            def _(way=way):
                all_rows(m, origin(way, k + 1), way, k, True).wait_send()
        return carry

    lax.fori_loop(0, 2 * last, finish, 0)
    pltpu.make_async_remote_copy(
        part.at[:, pl.ds(theirs, chips * share)], near, ss.at[0], sr.at[0],
        device_id=sibling, device_id_type=MESH).wait_send()
    for j in range(1, chips):
        pltpu.make_async_remote_copy(
            pair.at[:, chip(j)], far.at[:, j - 1], bs.at[j - 1], br.at[0],
            device_id=(g, f, 2 * chip(j) + c), device_id_type=MESH).wait_send()


def gather(n, tp, tokens, gain, up, down):
    local, width = up.shape
    count_rows = tokens.shape[0]
    half = local // 2
    block = divisor(half, 256, 16)
    rows = chunk_rows(block, width)
    count = half // rows
    depth = n * local
    piece = next(size for size in (512, 256, 128, width) if width % size == 0)
    moves = 2 * (n - 1) * count
    share, chips, total = count_rows // tp, tp // 2, depth // block
    dma = pltpu.SemaphoreType.DMA
    step_rows = divisor(local, 128, 8)
    sent = 3 * (n - 1) * local * width * 2
    anywhere = pl.BlockSpec(memory_space=pl.ANY)
    inside = pl.BlockSpec(memory_space=pltpu.VMEM)
    return pl.pallas_call(
        functools.partial(gather_kernel, (n, tp, local, block, rows, piece)),
        out_shape=[
            pltpu.VMEM((2, depth, width), jnp.bfloat16),
            pltpu.VMEM((total, share, block), jnp.bfloat16),
        ],
        in_specs=[anywhere, inside, anywhere, anywhere],
        out_specs=[inside, inside],
        scratch_shapes=[
            pltpu.VMEM((min(SLOTS, 4 * count), rows, width), jnp.float32),
            pltpu.VMEM((local, 1), jnp.float32),
            pltpu.VMEM((count_rows, depth), jnp.bfloat16),
            pltpu.VMEM((depth // block, count_rows, block), jnp.bfloat16),
            pltpu.VMEM((width // piece, count_rows, piece), jnp.float32),
            pltpu.VMEM((width // piece, count_rows, piece), jnp.bfloat16),
            pltpu.VMEM((5, count_rows, block), jnp.float32),
            pltpu.VMEM((total, count_rows, block), jnp.bfloat16),
            pltpu.VMEM((total, count_rows // 2, block), jnp.bfloat16),
            pltpu.VMEM((total, chips, share, block), jnp.bfloat16),
            pltpu.VMEM((total, share, block), jnp.float32),
            pltpu.VMEM((total, chips - 1, share, block), jnp.bfloat16),
            dma((min(SLOTS, 4 * count),)),
            dma((1,)),
            dma((4 * (n - 1),)),
            dma((2 * moves,)),
            dma((4 * (n - 1),)),
            dma((moves,)),
            dma((1,)),
            dma((total,)),
            dma((chips - 1,)),
            dma((total * (chips - 1),)),
        ],
        compiler_params=pltpu.CompilerParams(
            collective_id=0, has_side_effects=True, vmem_limit_bytes=27 * 512 * 1024),
        cost_estimate=pl.CostEstimate(flops=0, bytes_accessed=sent, transcendentals=0),
        name="gather_both",
    )(tokens, gain.reshape(local // step_rows, step_rows), up, down)


def write_kernel(parts, both, mixed, up_ready, down_ready, mixed_out, done):
    depth = both.shape[1]
    size = depth // parts
    copies = []
    for m, ready in enumerate((up_ready, down_ready)):
        for i in range(parts):
            place = pl.ds(i * size, size)
            copies.append(pltpu.make_async_copy(both.at[m, place], ready.at[place], done.at[m * parts + i]))
    for copy in copies:
        copy.start()
    block = mixed.shape[2]
    for i in range(mixed.shape[0]):
        mixed_out[:, i * block:(i + 1) * block] = mixed[i]
    for copy in copies:
        copy.wait()


def per_device(n, tp, tokens, norm_gain, up_master, down_master):
    both, mixed = gather(n, tp, tokens, norm_gain, up_master, down_master)
    depth, width = both.shape[1:]
    share = mixed.shape[1]
    weight = jax.ShapeDtypeStruct((depth, width), jnp.bfloat16)
    anywhere = pl.BlockSpec(memory_space=pl.ANY)
    inside = pl.BlockSpec(memory_space=pltpu.VMEM)
    parts = 8
    return tuple(pl.pallas_call(
        functools.partial(write_kernel, parts),
        out_shape=[weight, weight, jax.ShapeDtypeStruct((share, depth), jnp.bfloat16)],
        in_specs=[anywhere, inside],
        out_specs=[anywhere, anywhere, inside],
        scratch_shapes=[pltpu.SemaphoreType.DMA((2 * parts,))],
        compiler_params=pltpu.CompilerParams(vmem_limit_bytes=27 * 512 * 1024),
        name="write_out",
    )(pltpu.with_memory_space_constraint(both, pltpu.VMEM), pltpu.with_memory_space_constraint(mixed, pltpu.VMEM)))


def solution(mesh):
    n, tp = (mesh.shape[name] for name in ("fs", "tp"))
    return jax.shard_map(
        functools.partial(per_device, n, tp),
        mesh=mesh,
        in_specs=(P(("grp", "fs"), None), P("fs"), P("fs", "tp"), P("fs", "tp")),
        out_specs=(P("grp", "tp"), P("grp", "tp"), P(("grp", "fs", "tp"), None)),
        check_vma=False,
    )
```

```python
import functools

import jax
import jax.numpy as jnp
from jax import lax
from jax.experimental import pallas as pl
from jax.experimental.pallas import tpu as pltpu
from jax.sharding import PartitionSpec as P

MESH = pl.DeviceIdType.MESH
SLOTS = 6
LAG = 2


def divisor(total, most, least):
    for size in range(most, 0, -least):
        if total % size == 0:
            return size
    return total


def chunk_rows(block, width):
    for rows in range(16, block + 1, 16):
        if block % rows == 0 and rows * width * 2 >= 200 * 1024:
            return rows
    return block


def gather_kernel(sizes, tokens, gain, up, down, both, out, wide, column, held, normed, acc, hidden, product,
                  ending, part, far, load, token_s, zs, zr, xs, xr, ss, sr):
    n, tp, local, block, rows, piece = sizes
    half = local // 2
    count = half // rows
    per_block = block // rows
    blocks = half // block
    last = n - 1
    span = last * count
    total = 2 * span
    slots = wide.shape[0]
    g, f, t = lax.axis_index("grp"), lax.axis_index("fs"), lax.axis_index("tp")
    other = 1 - g
    every = 2 * blocks
    share = part.shape[2]
    final = total // per_block
    pieces = acc.shape[0]
    each = -(-pieces // per_block)
    double = jnp.minimum(f, last - f)

    def start_load(m, which, q, index):
        first = pl.multiple_of(which * half + q * rows, 16)
        slot = lax.rem(index, slots)
        pltpu.make_async_copy((up, down)[m].at[pl.ds(first, rows)], wide.at[slot], load.at[slot]).start()

    def next_load(index):
        @pl.when(index < count)
        def _():
            start_load(0, g, index, index)

        for m in range(2):
            @pl.when((index >= count) & (index < 3 * count) & (lax.rem(index + count, 2) == m))
            def _(m=m):
                start_load(m, other, lax.div(index - count, 2), index)

        @pl.when((index >= 3 * count) & (index < 4 * count))
        def _():
            start_load(1, g, index - 3 * count, index)

    def where(m, source, which, q):
        first = pl.multiple_of(source * local + which * half + q * rows, 16)
        return both.at[m, pl.ds(first, rows)]

    def convert(m, which, q, index):
        slot = lax.rem(index, slots)
        pltpu.make_async_copy(up.at[pl.ds(0, rows)], wide.at[slot], load.at[slot]).wait()
        near = pl.multiple_of(which * half + q * rows, 16)
        first = pl.multiple_of(f * local + which * half + q * rows, 16)
        values = wide[slot]
        if m == 0:
            values = column[pl.ds(near, rows)] * values
        both[m, pl.ds(first, rows)] = values.astype(jnp.bfloat16)
        next_load(index + slots)

    has = (f < last, f > 0)

    def hop(way):
        return (g, f + 1 if way == 0 else f - 1, t)

    def origin(way, k):
        return f - k if way == 0 else f + k

    def reach(way, k):
        return (k <= f) if way == 0 else (k <= last - f)

    def z_at(way, m, k, q):
        return ((way * 2 + m) * last + k) * count + q

    def along(way, m, k, q):
        place = where(m, origin(way, k), g, q)
        return pltpu.make_async_remote_copy(
            place, place, zs.at[(way * 2 + m) * last + k], zr.at[z_at(way, m, k, q)],
            device_id=hop(way), device_id_type=MESH)

    def all_rows(m, source, way, k, across_x):
        place = both.at[m, pl.ds(pl.multiple_of(source * local + g * half, 16), half)]
        at = (way * 2 + m) * last + k
        return pltpu.make_async_remote_copy(
            place, place, (xs if across_x else zs).at[at], zr.at[0],
            device_id=(other, f, t) if across_x else hop(way), device_id_type=MESH)

    def arrival(way, m, k, q):
        place = where(m, origin(way, k), g, q)
        return pltpu.make_async_remote_copy(
            place, place, zs.at[0], zr.at[z_at(way, m, k - 1, q)],
            device_id=hop(way), device_id_type=MESH)

    def x_at(way, m, k, q):
        two = k <= double
        base = jnp.where(two, 2 * count * (k - 1), count * (k - 1 + double))
        return m * span + base + jnp.where(two, 2 * q + way, q)

    def x_of(i):
        m, j = lax.div(i, span), lax.rem(i, span)
        two = j < 2 * count * double
        single = jnp.maximum(j - 2 * count * double, 0)
        k = jnp.where(two, 1 + lax.div(j, 2 * count), 1 + double + lax.div(single, count))
        q = jnp.where(two, lax.div(lax.rem(j, 2 * count), 2), lax.rem(single, count))
        up_side = jnp.where(two, lax.rem(j, 2), jnp.where(f < last - f, 1, 0))
        source = f + (2 * up_side - 1) * k
        return m, source, q

    def across(m, source, which, q, sent, i):
        place = where(m, source, which, q)
        return pltpu.make_async_remote_copy(
            place, place, xs.at[sent], xr.at[i], device_id=(other, f, t), device_id_type=MESH)

    def send_own(m, q):
        for way in range(2):
            @pl.when(has[way])
            def _(way=way):
                along(way, m, 0, q).start()

    lax.fori_loop(0, slots, lambda i, c: (next_load(i), c)[1], 0)
    token_copy = pltpu.make_async_copy(tokens, held, token_s.at[0])
    token_copy.start()

    barrier = pltpu.get_barrier_semaphore()
    for way in range(2):
        @pl.when(has[way])
        def _(way=way):
            pl.semaphore_signal(barrier, inc=1, device_id=hop(way), device_id_type=MESH)
    pl.semaphore_signal(barrier, inc=1, device_id=(other, f, t), device_id_type=MESH)

    def mate(j):
        return lax.rem(t + j, tp)

    for j in range(1, tp):
        pl.semaphore_signal(barrier, inc=1, device_id=(g, f, mate(j)), device_id_type=MESH)
    step_rows = divisor(local, 128, 8)
    eye = lax.broadcasted_iota(jnp.int32, (step_rows, step_rows), 0) == lax.broadcasted_iota(
        jnp.int32, (step_rows, step_rows), 1)
    for i in range(local // step_rows):
        line = gain[i:i + 1, :]
        column[i * step_rows:(i + 1) * step_rows, :] = jnp.sum(
            jnp.where(eye, line, 0.0), axis=1, keepdims=True)
    pl.semaphore_wait(barrier, tp + jnp.minimum(f, 1) + jnp.minimum(last - f, 1))

    def first_step(q, carry):
        convert(0, g, q, q)

        @pl.when(q > 0)
        def _():
            send_own(0, q - 1)
        return carry

    lax.fori_loop(0, count, first_step, 0)
    token_copy.wait()
    values = held[...].astype(jnp.float32)
    square_mean = jnp.mean(values * values, axis=1, keepdims=True)
    send_own(0, count - 1)
    scaled = (values * lax.rsqrt(square_mean + 1e-06)).astype(jnp.bfloat16)
    for i in range(normed.shape[0]):
        normed[i] = scaled[:, i * block:(i + 1) * block]
    acc[...] = jnp.zeros_like(acc)

    def slot_of(period, slot):
        i = period * per_block - 1
        m, j = lax.div(i, span), lax.rem(i, span)
        k, q = 1 + lax.div(j, count), lax.rem(j, count)
        z_block = g * blocks + lax.div(q, per_block)
        two = j < 2 * count * double
        single = jnp.maximum(j - 2 * count * double, 0)
        xk = jnp.where(two, 1 + lax.div(j, 2 * count), 1 + double + lax.div(single, count))
        xq = jnp.where(two, lax.div(lax.rem(j, 2 * count), 2), lax.rem(single, count))
        x_full = jnp.where(two, lax.rem(j, 2 * per_block) == 2 * per_block - 1, slot == 2)
        above = jnp.where(two, slot == 3, f < last - f)
        source = jnp.where(above, f + xk, f - xk)
        own = lax.div(j + 1 - count, per_block)
        exists = (period > 0) & jnp.where(
            slot == 0, k <= f, jnp.where(
                slot == 1, k <= last - f, jnp.where(
                    slot == 4, (j + 1 >= count) & (own < every), x_full)))
        index = jnp.where(
            slot == 0, (f - k) * every + z_block, jnp.where(
                slot == 1, (f + k) * every + z_block, jnp.where(
                    slot == 4, f * every + own,
                    source * every + other * blocks + lax.div(xq, per_block))))
        return exists, m, index

    def multiply(m, index, slot, p):
        first = pl.multiple_of(index * block, 16)
        at = pl.multiple_of(p * piece, piece)

        @pl.when(m == 0)
        def _():
            acc[p] += jnp.dot(
                normed[index], both[0, pl.ds(first, block), pl.ds(at, piece)],
                preferred_element_type=jnp.float32)

        @pl.when(m == 1)
        def _():
            value = lax.dot_general(
                hidden[p], both[1, pl.ds(first, block), pl.ds(at, piece)],
                (((1,), (1,)), ((), ())), preferred_element_type=jnp.float32)

            @pl.when(p == 0)
            def _():
                product[slot] = value

            @pl.when(p > 0)
            def _():
                product[slot] += value

    def share_out(index, j):
        at = index * (tp - 1) + j - 1
        return pltpu.make_async_remote_copy(
            part.at[index, mate(j)], far.at[index, j - 1], ss.at[j - 1], sr.at[at],
            device_id=(g, f, mate(j)), device_id_type=MESH)

    def stage(which, period, low=0, high=5):
        def one(slot, carry):
            exists, m, index = slot_of(period, slot)

            @pl.when(exists & (m == 1))
            def _():
                if which == 0:
                    for j in range(tp):
                        part[index, j] = product[slot, j * share:(j + 1) * share].astype(jnp.bfloat16)
                elif which == 1:
                    for j in range(1, tp):
                        share_out(index, j).start()
                else:
                    value = part[index, t].astype(jnp.float32)
                    for j in range(1, tp):
                        share_out(index, j).wait_recv()
                        value = value + far[index, j - 1].astype(jnp.float32)
                    out[index] = value.astype(jnp.bfloat16)
            return carry

        lax.fori_loop(low, high, one, 0)

    def forward(s):
        m, j = lax.div(s, span), lax.rem(s, span)
        k, q = 1 + lax.div(j, count), lax.rem(j, count)

        @pl.when(s < count)
        def _():
            for w in range(2):
                convert(w, other, s, count + 2 * s + w)

        @pl.when((s >= span - count) & (s < span))
        def _():
            convert(1, g, s - (span - count), 3 * count + s - (span - count))

        @pl.when((s > span - count) & (s <= span))
        def _():
            send_own(1, s - 1 - (span - count))

        for way in range(2):
            @pl.when(reach(way, k))
            def _(way=way):
                arrival(way, m, k, q).wait_recv()

                @pl.when(has[way])
                def _():
                    along(way, m, k, q).start()
                across(
                    m, origin(way, k), g, q, (way * 2 + m) * last + k - 1, x_at(way, m, k, q)).start()

    def run(period, low, high, first, end):
        def one(slot, carry):
            exists, m, index = slot_of(period, slot)

            @pl.when(exists)
            def _():
                def body(r, carry):
                    multiply(m, index, slot, r)
                    return carry
                lax.fori_loop(first, end, body, 0)
            return carry

        lax.fori_loop(low, high, one, 0)

    def absorb(i, low, high, wait):
        if wait:
            _, source, xq = x_of(i)
            across(0, source, other, xq, 0, i).wait_recv()

            @pl.when((i >= total - per_block) & (n % 2 == 0))
            def _():
                first = pl.multiple_of(source * local + other * half + xq * rows, 16)
                value = jnp.zeros(ending.shape[1:], jnp.float32)
                for p in range(pieces):
                    value = value + lax.dot_general(
                        hidden[p], both[1, pl.ds(first, rows), p * piece:(p + 1) * piece],
                        (((1,), (1,)), ((), ())), preferred_element_type=jnp.float32)
                ending[lax.rem(i, per_block)] = value
        period, p = lax.div(i, per_block), lax.rem(i, per_block)
        run(period, low, high, jnp.minimum(p * each, pieces), jnp.minimum((p + 1) * each, pieces))

        @pl.when(p == per_block - 1)
        def _():
            stage(0, period, low, high)
            stage(1, period, low, high)
            if wait:
                stage(2, period - 1)

        if wait:
            @pl.when(i == span + per_block - 1)
            def _():
                for r in range(pieces):
                    hidden[r] = jnp.square(jnp.maximum(acc[r], 0.0)).astype(jnp.bfloat16)

    def step(s, carry):
        forward(s)

        @pl.when(s >= LAG)
        def _():
            absorb(s - LAG, 0, 5, True)
        return carry

    lax.fori_loop(0, total, step, 0)
    def drain(low, high, wait):
        def one(i, carry):
            absorb(i, low, high, wait)
            return carry

        lax.fori_loop(total - LAG, total, one, 0)

    drain(0, 2, False)
    run(final, 0, 2, 0, pieces)
    stage(0, final, 0, 2)
    stage(1, final, 0, 2)
    drain(2, 5, True)
    if n % 2 == 0:
        for p in range(per_block):
            product[2, :, p * rows:(p + 1) * rows] = ending[p]
    else:
        run(final, 2, 4, 0, pieces)
    stage(0, final, 2, 4)
    stage(1, final, 2, 4)
    stage(2, final - 1)
    stage(2, final, 0, 4)

    def finish(r, carry):
        m, k = lax.div(r, last), lax.rem(r, last)
        for way in range(2):
            @pl.when(has[way] & ((k == 0) | reach(way, k)))
            def _(way=way):
                all_rows(m, origin(way, k), way, k, False).wait_send()

            @pl.when(reach(way, k + 1))
            def _(way=way):
                all_rows(m, origin(way, k + 1), way, k, True).wait_send()
        return carry

    lax.fori_loop(0, 2 * last, finish, 0)
    for j in range(1, tp):
        pltpu.make_async_remote_copy(
            part.at[:, mate(j)], far.at[:, j - 1], ss.at[j - 1], sr.at[0],
            device_id=(g, f, mate(j)), device_id_type=MESH).wait_send()


def gather(n, tp, tokens, gain, up, down):
    local, width = up.shape
    count_rows = tokens.shape[0]
    half = local // 2
    block = divisor(half, 256, 16)
    rows = chunk_rows(block, width)
    count = half // rows
    depth = n * local
    piece = next(size for size in (512, 256, 128, width) if width % size == 0)
    moves = 2 * (n - 1) * count
    share, total = count_rows // tp, depth // block
    dma = pltpu.SemaphoreType.DMA
    step_rows = divisor(local, 128, 8)
    sent = 3 * (n - 1) * local * width * 2
    anywhere = pl.BlockSpec(memory_space=pl.ANY)
    inside = pl.BlockSpec(memory_space=pltpu.VMEM)
    return pl.pallas_call(
        functools.partial(gather_kernel, (n, tp, local, block, rows, piece)),
        out_shape=[
            pltpu.VMEM((2, depth, width), jnp.bfloat16),
            pltpu.VMEM((total, share, block), jnp.bfloat16),
        ],
        in_specs=[anywhere, inside, anywhere, anywhere],
        out_specs=[inside, inside],
        scratch_shapes=[
            pltpu.VMEM((min(SLOTS, 4 * count), rows, width), jnp.float32),
            pltpu.VMEM((local, 1), jnp.float32),
            pltpu.VMEM((count_rows, depth), jnp.bfloat16),
            pltpu.VMEM((depth // block, count_rows, block), jnp.bfloat16),
            pltpu.VMEM((width // piece, count_rows, piece), jnp.float32),
            pltpu.VMEM((width // piece, count_rows, piece), jnp.bfloat16),
            pltpu.VMEM((5, count_rows, block), jnp.float32),
            pltpu.VMEM((block // rows, count_rows, rows), jnp.float32),
            pltpu.VMEM((total, tp, share, block), jnp.bfloat16),
            pltpu.VMEM((total, tp - 1, share, block), jnp.bfloat16),
            dma((min(SLOTS, 4 * count),)),
            dma((1,)),
            dma((4 * (n - 1),)),
            dma((2 * moves,)),
            dma((4 * (n - 1),)),
            dma((moves,)),
            dma((tp - 1,)),
            dma((total * (tp - 1),)),
        ],
        compiler_params=pltpu.CompilerParams(
            collective_id=0, has_side_effects=True, vmem_limit_bytes=27 * 512 * 1024),
        cost_estimate=pl.CostEstimate(flops=0, bytes_accessed=sent, transcendentals=0),
        name="gather_both",
    )(tokens, gain.reshape(local // step_rows, step_rows), up, down)


def write_kernel(parts, both, mixed, up_ready, down_ready, mixed_out, done):
    depth = both.shape[1]
    size = depth // parts
    copies = []
    for m, ready in enumerate((up_ready, down_ready)):
        for i in range(parts):
            place = pl.ds(i * size, size)
            copies.append(pltpu.make_async_copy(both.at[m, place], ready.at[place], done.at[m * parts + i]))
    for copy in copies:
        copy.start()
    block = mixed.shape[2]
    for i in range(mixed.shape[0]):
        mixed_out[:, i * block:(i + 1) * block] = mixed[i]
    for copy in copies:
        copy.wait()


def per_device(n, tp, tokens, norm_gain, up_master, down_master):
    both, mixed = gather(n, tp, tokens, norm_gain, up_master, down_master)
    depth, width = both.shape[1:]
    share = mixed.shape[1]
    weight = jax.ShapeDtypeStruct((depth, width), jnp.bfloat16)
    anywhere = pl.BlockSpec(memory_space=pl.ANY)
    inside = pl.BlockSpec(memory_space=pltpu.VMEM)
    parts = 8
    return tuple(pl.pallas_call(
        functools.partial(write_kernel, parts),
        out_shape=[weight, weight, jax.ShapeDtypeStruct((share, depth), jnp.bfloat16)],
        in_specs=[anywhere, inside],
        out_specs=[anywhere, anywhere, inside],
        scratch_shapes=[pltpu.SemaphoreType.DMA((2 * parts,))],
        compiler_params=pltpu.CompilerParams(vmem_limit_bytes=27 * 512 * 1024),
        name="write_out",
    )(pltpu.with_memory_space_constraint(both, pltpu.VMEM), pltpu.with_memory_space_constraint(mixed, pltpu.VMEM)))


def solution(mesh):
    n, tp = (mesh.shape[name] for name in ("fs", "tp"))
    return jax.shard_map(
        functools.partial(per_device, n, tp),
        mesh=mesh,
        in_specs=(P(("grp", "fs"), None), P("fs"), P("fs", "tp"), P("fs", "tp")),
        out_specs=(P("grp", "tp"), P("grp", "tp"), P(("grp", "fs", "tp"), None)),
        check_vma=False,
    )
```

```python
import functools

import jax
import jax.numpy as jnp
from jax import lax
from jax.experimental import pallas as pl
from jax.experimental.pallas import tpu as pltpu
from jax.sharding import PartitionSpec as P

MESH = pl.DeviceIdType.MESH
SLOTS = 6
LAG = 2


def divisor(total, most, least):
    for size in range(most, 0, -least):
        if total % size == 0:
            return size
    return total


def chunk_rows(block, width):
    for rows in range(16, block + 1, 16):
        if block % rows == 0 and rows * width * 2 >= 200 * 1024:
            return rows
    return block


def gather_kernel(sizes, tokens, gain, up, down, both, out, wide, column, held, normed, acc, hidden, product,
                  ending, part, far, load, token_s, zs, zr, xs, xr, es, er, ss, sr):
    n, tp, local, block, rows, piece = sizes
    half = local // 2
    count = half // rows
    per_block = block // rows
    blocks = half // block
    last = n - 1
    span = last * count
    total = 2 * span
    slots = wide.shape[0]
    g, f, t = lax.axis_index("grp"), lax.axis_index("fs"), lax.axis_index("tp")
    other = 1 - g
    every = 2 * blocks
    share = part.shape[2]
    final = total // per_block
    extra = rows // 32 * 16
    pieces = acc.shape[0]
    each = -(-pieces // per_block)
    double = jnp.minimum(f, last - f)

    def start_load(m, which, q, index):
        first = pl.multiple_of(which * half + q * rows, 16)
        slot = lax.rem(index, slots)
        pltpu.make_async_copy((up, down)[m].at[pl.ds(first, rows)], wide.at[slot], load.at[slot]).start()

    def next_load(index):
        @pl.when(index < count)
        def _():
            start_load(0, g, index, index)

        for m in range(2):
            @pl.when((index >= count) & (index < 3 * count) & (lax.rem(index + count, 2) == m))
            def _(m=m):
                start_load(m, other, lax.div(index - count, 2), index)

        @pl.when((index >= 3 * count) & (index < 4 * count))
        def _():
            start_load(1, g, index - 3 * count, index)

    def where(m, source, which, q):
        first = pl.multiple_of(source * local + which * half + q * rows, 16)
        return both.at[m, pl.ds(first, rows)]

    def convert(m, which, q, index):
        slot = lax.rem(index, slots)
        pltpu.make_async_copy(up.at[pl.ds(0, rows)], wide.at[slot], load.at[slot]).wait()
        near = pl.multiple_of(which * half + q * rows, 16)
        first = pl.multiple_of(f * local + which * half + q * rows, 16)
        values = wide[slot]
        if m == 0:
            values = column[pl.ds(near, rows)] * values
        both[m, pl.ds(first, rows)] = values.astype(jnp.bfloat16)
        next_load(index + slots)

    has = (f < last, f > 0)

    def hop(way):
        return (g, f + 1 if way == 0 else f - 1, t)

    def origin(way, k):
        return f - k if way == 0 else f + k

    def reach(way, k):
        return (k <= f) if way == 0 else (k <= last - f)

    def z_at(way, m, k, q):
        return ((way * 2 + m) * last + k) * count + q

    def along(way, m, k, q):
        place = where(m, origin(way, k), g, q)
        return pltpu.make_async_remote_copy(
            place, place, zs.at[(way * 2 + m) * last + k], zr.at[z_at(way, m, k, q)],
            device_id=hop(way), device_id_type=MESH)

    ends = (0, last)

    def shortened(m, source, q):
        return (m == 1) & (q == count - 1) & ((source == 0) | (source == last)) & (extra > 0)

    def extra_rows(way, source):
        first = pl.multiple_of(source * local + other * half + half - extra, 16)
        place = both.at[1, pl.ds(first, extra)]
        return pltpu.make_async_remote_copy(
            place, place, es.at[way], er.at[way], device_id=hop(way), device_id_type=MESH)

    def all_rows(m, source, way, k, across_x, size):
        place = both.at[m, pl.ds(pl.multiple_of(source * local + g * half, 16), size)]
        at = (way * 2 + m) * last + k
        return pltpu.make_async_remote_copy(
            place, place, (xs if across_x else zs).at[at], zr.at[0],
            device_id=(other, f, t) if across_x else hop(way), device_id_type=MESH)

    def arrival(way, m, k, q):
        place = where(m, origin(way, k), g, q)
        return pltpu.make_async_remote_copy(
            place, place, zs.at[0], zr.at[z_at(way, m, k - 1, q)],
            device_id=hop(way), device_id_type=MESH)

    def x_at(way, m, k, q):
        two = k <= double
        base = jnp.where(two, 2 * count * (k - 1), count * (k - 1 + double))
        return m * span + base + jnp.where(two, 2 * q + way, q)

    def x_of(i):
        m, j = lax.div(i, span), lax.rem(i, span)
        two = j < 2 * count * double
        single = jnp.maximum(j - 2 * count * double, 0)
        k = jnp.where(two, 1 + lax.div(j, 2 * count), 1 + double + lax.div(single, count))
        q = jnp.where(two, lax.div(lax.rem(j, 2 * count), 2), lax.rem(single, count))
        up_side = jnp.where(two, lax.rem(j, 2), jnp.where(f < last - f, 1, 0))
        source = f + (2 * up_side - 1) * k
        return m, source, q

    def across(m, source, which, q, sent, i, size=rows):
        first = pl.multiple_of(source * local + which * half + q * rows, 16)
        place = both.at[m, pl.ds(first, size)]
        return pltpu.make_async_remote_copy(
            place, place, xs.at[sent], xr.at[i], device_id=(other, f, t), device_id_type=MESH)

    def send_own(m, q):
        for way in range(2):
            @pl.when(has[way])
            def _(way=way):
                along(way, m, 0, q).start()

    lax.fori_loop(0, slots, lambda i, c: (next_load(i), c)[1], 0)
    token_copy = pltpu.make_async_copy(tokens, held, token_s.at[0])
    token_copy.start()

    barrier = pltpu.get_barrier_semaphore()
    for way in range(2):
        @pl.when(has[way])
        def _(way=way):
            pl.semaphore_signal(barrier, inc=1, device_id=hop(way), device_id_type=MESH)
    pl.semaphore_signal(barrier, inc=1, device_id=(other, f, t), device_id_type=MESH)

    def mate(j):
        return lax.rem(t + j, tp)

    for j in range(1, tp):
        pl.semaphore_signal(barrier, inc=1, device_id=(g, f, mate(j)), device_id_type=MESH)
    step_rows = divisor(local, 128, 8)
    eye = lax.broadcasted_iota(jnp.int32, (step_rows, step_rows), 0) == lax.broadcasted_iota(
        jnp.int32, (step_rows, step_rows), 1)
    for i in range(local // step_rows):
        line = gain[i:i + 1, :]
        column[i * step_rows:(i + 1) * step_rows, :] = jnp.sum(
            jnp.where(eye, line, 0.0), axis=1, keepdims=True)
    pl.semaphore_wait(barrier, tp + jnp.minimum(f, 1) + jnp.minimum(last - f, 1))

    def first_step(q, carry):
        convert(0, g, q, q)

        @pl.when(q > 0)
        def _():
            send_own(0, q - 1)
        return carry

    lax.fori_loop(0, count, first_step, 0)
    token_copy.wait()
    values = held[...].astype(jnp.float32)
    square_mean = jnp.mean(values * values, axis=1, keepdims=True)
    send_own(0, count - 1)
    scaled = (values * lax.rsqrt(square_mean + 1e-06)).astype(jnp.bfloat16)
    for i in range(normed.shape[0]):
        normed[i] = scaled[:, i * block:(i + 1) * block]
    acc[...] = jnp.zeros_like(acc)

    def slot_of(period, slot):
        i = period * per_block - 1
        m, j = lax.div(i, span), lax.rem(i, span)
        k, q = 1 + lax.div(j, count), lax.rem(j, count)
        z_block = g * blocks + lax.div(q, per_block)
        two = j < 2 * count * double
        single = jnp.maximum(j - 2 * count * double, 0)
        xk = jnp.where(two, 1 + lax.div(j, 2 * count), 1 + double + lax.div(single, count))
        xq = jnp.where(two, lax.div(lax.rem(j, 2 * count), 2), lax.rem(single, count))
        x_full = jnp.where(two, lax.rem(j, 2 * per_block) == 2 * per_block - 1, slot == 2)
        above = jnp.where(two, slot == 3, f < last - f)
        source = jnp.where(above, f + xk, f - xk)
        own = lax.div(j + 1 - count, per_block)
        exists = (period > 0) & jnp.where(
            slot == 0, k <= f, jnp.where(
                slot == 1, k <= last - f, jnp.where(
                    slot == 4, (j + 1 >= count) & (own < every), x_full)))
        index = jnp.where(
            slot == 0, (f - k) * every + z_block, jnp.where(
                slot == 1, (f + k) * every + z_block, jnp.where(
                    slot == 4, f * every + own,
                    source * every + other * blocks + lax.div(xq, per_block))))
        return exists, m, index

    def multiply(m, index, slot, p):
        first = pl.multiple_of(index * block, 16)
        at = pl.multiple_of(p * piece, piece)

        @pl.when(m == 0)
        def _():
            acc[p] += jnp.dot(
                normed[index], both[0, pl.ds(first, block), pl.ds(at, piece)],
                preferred_element_type=jnp.float32)

        @pl.when(m == 1)
        def _():
            value = lax.dot_general(
                hidden[p], both[1, pl.ds(first, block), pl.ds(at, piece)],
                (((1,), (1,)), ((), ())), preferred_element_type=jnp.float32)

            @pl.when(p == 0)
            def _():
                product[slot] = value

            @pl.when(p > 0)
            def _():
                product[slot] += value

    def share_out(index, j):
        at = index * (tp - 1) + j - 1
        return pltpu.make_async_remote_copy(
            part.at[index, mate(j)], far.at[index, j - 1], ss.at[j - 1], sr.at[at],
            device_id=(g, f, mate(j)), device_id_type=MESH)

    def stage(which, period, low=0, high=5):
        def one(slot, carry):
            exists, m, index = slot_of(period, slot)

            @pl.when(exists & (m == 1))
            def _():
                if which == 0:
                    for j in range(tp):
                        part[index, j] = product[slot, j * share:(j + 1) * share].astype(jnp.bfloat16)
                elif which == 1:
                    for j in range(1, tp):
                        share_out(index, j).start()
                else:
                    value = part[index, t].astype(jnp.float32)
                    for j in range(1, tp):
                        share_out(index, j).wait_recv()
                        value = value + far[index, j - 1].astype(jnp.float32)
                    out[index] = value.astype(jnp.bfloat16)
            return carry

        lax.fori_loop(low, high, one, 0)

    def forward(s):
        m, j = lax.div(s, span), lax.rem(s, span)
        k, q = 1 + lax.div(j, count), lax.rem(j, count)

        @pl.when(s < count)
        def _():
            for w in range(2):
                convert(w, other, s, count + 2 * s + w)

        @pl.when((s >= span - count) & (s < span))
        def _():
            convert(1, g, s - (span - count), 3 * count + s - (span - count))

        @pl.when((s > span - count) & (s <= span))
        def _():
            send_own(1, s - 1 - (span - count))

        if extra:
            for way in range(2):
                @pl.when((s == span) & (f == ends[way]))
                def _(way=way):
                    extra_rows(way, f).start()

        for way in range(2):
            @pl.when(reach(way, k))
            def _(way=way):
                arrival(way, m, k, q).wait_recv()

                @pl.when(has[way])
                def _():
                    along(way, m, k, q).start()
                short = shortened(m, origin(way, k), q)
                for size, chosen in ((rows, ~short), (rows - extra, short)):
                    @pl.when(chosen)
                    def _(size=size):
                        across(
                            m, origin(way, k), g, q, (way * 2 + m) * last + k - 1,
                            x_at(way, m, k, q), size).start()

        if extra:
            for way in range(2):
                @pl.when((m == 1) & (q == count - 1) & reach(way, k) & (origin(way, k) == ends[way]))
                def _(way=way):
                    extra_rows(way, ends[way]).wait_recv()

                    @pl.when(has[way])
                    def _():
                        extra_rows(way, ends[way]).start()

    def run(period, low, high, first, end):
        def one(slot, carry):
            exists, m, index = slot_of(period, slot)

            @pl.when(exists)
            def _():
                def body(r, carry):
                    multiply(m, index, slot, r)
                    return carry
                lax.fori_loop(first, end, body, 0)
            return carry

        lax.fori_loop(low, high, one, 0)

    def take(i):
        m = lax.div(i, span)
        _, source, xq = x_of(i)
        short = shortened(m, source, xq)
        for size, chosen in ((rows, ~short), (rows - extra, short)):
            @pl.when(chosen)
            def _(size=size):
                across(0, source, other, xq, 0, i, size).wait_recv()
        return source, xq

    def chunk_product(source, xq):
        first = pl.multiple_of(source * local + other * half + xq * rows, 16)
        value = jnp.zeros(ending.shape[1:], jnp.float32)
        for p in range(pieces):
            value = value + lax.dot_general(
                hidden[p], both[1, pl.ds(first, rows), p * piece:(p + 1) * piece],
                (((1,), (1,)), ((), ())), preferred_element_type=jnp.float32)
        return value

    single = n % 2 == 0

    def take_and_multiply(i):
        source, xq = take(i)
        if single:
            @pl.when(i >= total - per_block)
            def _():
                ending[lax.rem(i, per_block)] = chunk_product(source, xq)

    def absorb(i, low, high, wait):
        if wait:
            take_and_multiply(i)
        rest(i, low, high, wait)

    def rest(i, low, high, wait):
        period, p = lax.div(i, per_block), lax.rem(i, per_block)
        run(period, low, high, jnp.minimum(p * each, pieces), jnp.minimum((p + 1) * each, pieces))

        @pl.when(p == per_block - 1)
        def _():
            stage(0, period, low, high)
            stage(1, period, low, high)
            if wait:
                stage(2, period - 1)

        if wait:
            @pl.when(i == span + per_block - 1)
            def _():
                for r in range(pieces):
                    hidden[r] = jnp.square(jnp.maximum(acc[r], 0.0)).astype(jnp.bfloat16)

    def step(s, carry):
        forward(s)

        @pl.when(s >= LAG)
        def _():
            absorb(s - LAG, 0, 5, True)
        return carry

    lax.fori_loop(0, total, step, 0)
    def drain(low, high, wait, end):
        def one(i, carry):
            absorb(i, low, high, wait)
            return carry

        lax.fori_loop(total - LAG, end, one, 0)

    def finish(r, carry):
        m, k = lax.div(r, last), lax.rem(r, last)
        for way in range(2):
            @pl.when(has[way] & ((k == 0) | reach(way, k)))
            def _(way=way):
                all_rows(m, origin(way, k), way, k, False, half).wait_send()

            short = shortened(m, origin(way, k + 1), count - 1)
            for size, chosen in ((half, ~short), (half - extra, short)):
                @pl.when(reach(way, k + 1) & chosen)
                def _(way=way, size=size):
                    all_rows(m, origin(way, k + 1), way, k, True, size).wait_send()
        return carry

    def finish_all():
        lax.fori_loop(0, 2 * last, finish, 0)
        if extra:
            for way in range(2):
                @pl.when(has[way])
                def _(way=way):
                    extra_rows(way, ends[way]).wait_send()

    drain(0, 2, False, total)
    run(final, 0, 2, 0, pieces)
    stage(0, final, 0, 2)
    stage(1, final, 0, 2)
    if single:
        drain(2, 5, True, total - 1)
        rest(total - 1, 2, 5, True)
        stage(2, final - 1)
        _, source, _ = x_of(total - 1)
        index = source * every + other * blocks + blocks - 1
        for p in range(per_block - 1):
            value = ending[p].astype(jnp.bfloat16)
            for j in range(tp):
                part[index, j, :, p * rows:(p + 1) * rows] = value[j * share:(j + 1) * share]
        take(total - 1)
        value = chunk_product(source, count - 1).astype(jnp.bfloat16)
        for j in range(tp):
            part[index, j, :, (per_block - 1) * rows:] = value[j * share:(j + 1) * share]
        for j in range(1, tp):
            share_out(index, j).start()
        finish_all()
        stage(2, final, 0, 2)
        value = part[index, t].astype(jnp.float32)
        for j in range(1, tp):
            share_out(index, j).wait_recv()
            value = value + far[index, j - 1].astype(jnp.float32)
        out[index] = value.astype(jnp.bfloat16)
    else:
        drain(2, 5, True, total)
        run(final, 2, 4, 0, pieces)
        stage(0, final, 2, 4)
        stage(1, final, 2, 4)
        finish_all()
        stage(2, final - 1)
        stage(2, final, 0, 4)
    for j in range(1, tp):
        pltpu.make_async_remote_copy(
            part.at[:, mate(j)], far.at[:, j - 1], ss.at[j - 1], sr.at[0],
            device_id=(g, f, mate(j)), device_id_type=MESH).wait_send()


def gather(n, tp, tokens, gain, up, down):
    local, width = up.shape
    count_rows = tokens.shape[0]
    half = local // 2
    block = divisor(half, 256, 16)
    rows = chunk_rows(block, width)
    count = half // rows
    depth = n * local
    piece = next(size for size in (512, 256, 128, width) if width % size == 0)
    moves = 2 * (n - 1) * count
    share, total = count_rows // tp, depth // block
    dma = pltpu.SemaphoreType.DMA
    step_rows = divisor(local, 128, 8)
    sent = 3 * (n - 1) * local * width * 2
    anywhere = pl.BlockSpec(memory_space=pl.ANY)
    inside = pl.BlockSpec(memory_space=pltpu.VMEM)
    return pl.pallas_call(
        functools.partial(gather_kernel, (n, tp, local, block, rows, piece)),
        out_shape=[
            pltpu.VMEM((2, depth, width), jnp.bfloat16),
            pltpu.VMEM((total, share, block), jnp.bfloat16),
        ],
        in_specs=[anywhere, inside, anywhere, anywhere],
        out_specs=[inside, inside],
        scratch_shapes=[
            pltpu.VMEM((min(SLOTS, 4 * count), rows, width), jnp.float32),
            pltpu.VMEM((local, 1), jnp.float32),
            pltpu.VMEM((count_rows, depth), jnp.bfloat16),
            pltpu.VMEM((depth // block, count_rows, block), jnp.bfloat16),
            pltpu.VMEM((width // piece, count_rows, piece), jnp.float32),
            pltpu.VMEM((width // piece, count_rows, piece), jnp.bfloat16),
            pltpu.VMEM((5, count_rows, block), jnp.float32),
            pltpu.VMEM((block // rows, count_rows, rows), jnp.float32),
            pltpu.VMEM((total, tp, share, block), jnp.bfloat16),
            pltpu.VMEM((total, tp - 1, share, block), jnp.bfloat16),
            dma((min(SLOTS, 4 * count),)),
            dma((1,)),
            dma((4 * (n - 1),)),
            dma((2 * moves,)),
            dma((4 * (n - 1),)),
            dma((moves,)),
            dma((2,)),
            dma((2,)),
            dma((tp - 1,)),
            dma((total * (tp - 1),)),
        ],
        compiler_params=pltpu.CompilerParams(
            collective_id=0, has_side_effects=True, vmem_limit_bytes=27 * 512 * 1024),
        cost_estimate=pl.CostEstimate(flops=0, bytes_accessed=sent, transcendentals=0),
        name="gather_both",
    )(tokens, gain.reshape(local // step_rows, step_rows), up, down)


def write_kernel(parts, both, mixed, up_ready, down_ready, mixed_out, done):
    depth = both.shape[1]
    size = depth // parts
    copies = []
    for m, ready in enumerate((up_ready, down_ready)):
        for i in range(parts):
            place = pl.ds(i * size, size)
            copies.append(pltpu.make_async_copy(both.at[m, place], ready.at[place], done.at[m * parts + i]))
    for copy in copies:
        copy.start()
    block = mixed.shape[2]
    for i in range(mixed.shape[0]):
        mixed_out[:, i * block:(i + 1) * block] = mixed[i]
    for copy in copies:
        copy.wait()


def per_device(n, tp, tokens, norm_gain, up_master, down_master):
    both, mixed = gather(n, tp, tokens, norm_gain, up_master, down_master)
    depth, width = both.shape[1:]
    share = mixed.shape[1]
    weight = jax.ShapeDtypeStruct((depth, width), jnp.bfloat16)
    anywhere = pl.BlockSpec(memory_space=pl.ANY)
    inside = pl.BlockSpec(memory_space=pltpu.VMEM)
    parts = 8
    return tuple(pl.pallas_call(
        functools.partial(write_kernel, parts),
        out_shape=[weight, weight, jax.ShapeDtypeStruct((share, depth), jnp.bfloat16)],
        in_specs=[anywhere, inside],
        out_specs=[anywhere, anywhere, inside],
        scratch_shapes=[pltpu.SemaphoreType.DMA((2 * parts,))],
        compiler_params=pltpu.CompilerParams(vmem_limit_bytes=27 * 512 * 1024),
        name="write_out",
    )(pltpu.with_memory_space_constraint(both, pltpu.VMEM), pltpu.with_memory_space_constraint(mixed, pltpu.VMEM)))


def solution(mesh):
    n, tp = (mesh.shape[name] for name in ("fs", "tp"))
    return jax.shard_map(
        functools.partial(per_device, n, tp),
        mesh=mesh,
        in_specs=(P(("grp", "fs"), None), P("fs"), P("fs", "tp"), P("fs", "tp")),
        out_specs=(P("grp", "tp"), P("grp", "tp"), P(("grp", "fs", "tp"), None)),
        check_vma=False,
    )
```

```python
import functools

import jax
import jax.numpy as jnp
from jax import lax
from jax.experimental import pallas as pl
from jax.experimental.pallas import tpu as pltpu
from jax.sharding import PartitionSpec as P

MESH = pl.DeviceIdType.MESH
SLOTS = 6
LAG = 2


def divisor(total, most, least):
    for size in range(most, 0, -least):
        if total % size == 0:
            return size
    return total


def chunk_rows(block, width):
    for rows in range(16, block + 1, 16):
        if block % rows == 0 and rows * width * 2 >= 200 * 1024:
            return rows
    return block


def gather_kernel(sizes, tokens, gain, up, down, both, out, wide, column, held, normed, acc, hidden, product,
                  ending, part, far, load, token_s, zs, zr, xs, xr, es, er, ss, sr):
    n, tp, local, block, rows, piece = sizes
    half = local // 2
    count = half // rows
    per_block = block // rows
    blocks = half // block
    last = n - 1
    span = last * count
    total = 2 * span
    slots = wide.shape[0]
    g, f, t = lax.axis_index("grp"), lax.axis_index("fs"), lax.axis_index("tp")
    other = 1 - g
    every = 2 * blocks
    share = part.shape[2]
    final = total // per_block
    extra = rows // 32 * 16
    pieces = acc.shape[0]
    trigger = per_block - 1 - LAG if per_block > 2 * LAG else per_block - 1
    each = -(-pieces // (trigger + 1))
    single = n % 2 == 0
    double = jnp.minimum(f, last - f)

    def start_load(m, which, q, index):
        first = pl.multiple_of(which * half + q * rows, 16)
        slot = lax.rem(index, slots)
        pltpu.make_async_copy((up, down)[m].at[pl.ds(first, rows)], wide.at[slot], load.at[slot]).start()

    def next_load(index):
        @pl.when(index < count)
        def _():
            start_load(0, g, index, index)

        for m in range(2):
            @pl.when((index >= count) & (index < 3 * count) & (lax.rem(index + count, 2) == m))
            def _(m=m):
                start_load(m, other, lax.div(index - count, 2), index)

        @pl.when((index >= 3 * count) & (index < 4 * count))
        def _():
            start_load(1, g, index - 3 * count, index)

    def where(m, source, which, q):
        first = pl.multiple_of(source * local + which * half + q * rows, 16)
        return both.at[m, pl.ds(first, rows)]

    def convert(m, which, q, index):
        slot = lax.rem(index, slots)
        pltpu.make_async_copy(up.at[pl.ds(0, rows)], wide.at[slot], load.at[slot]).wait()
        near = pl.multiple_of(which * half + q * rows, 16)
        first = pl.multiple_of(f * local + which * half + q * rows, 16)
        values = wide[slot]
        if m == 0:
            values = column[pl.ds(near, rows)] * values
        both[m, pl.ds(first, rows)] = values.astype(jnp.bfloat16)
        next_load(index + slots)

    has = (f < last, f > 0)

    def hop(way):
        return (g, f + 1 if way == 0 else f - 1, t)

    def origin(way, k):
        return f - k if way == 0 else f + k

    def reach(way, k):
        return (k <= f) if way == 0 else (k <= last - f)

    def z_at(way, m, k, q):
        return ((way * 2 + m) * last + k) * count + q

    def along(way, m, k, q):
        place = where(m, origin(way, k), g, q)
        return pltpu.make_async_remote_copy(
            place, place, zs.at[(way * 2 + m) * last + k], zr.at[z_at(way, m, k, q)],
            device_id=hop(way), device_id_type=MESH)

    ends = (0, last)

    def shortened(m, source, q):
        return (m == 1) & (q == count - 1) & ((source == 0) | (source == last)) & (extra > 0)

    def extra_rows(way, source):
        first = pl.multiple_of(source * local + other * half + half - extra, 16)
        place = both.at[1, pl.ds(first, extra)]
        return pltpu.make_async_remote_copy(
            place, place, es.at[way], er.at[way], device_id=hop(way), device_id_type=MESH)

    def all_rows(m, source, way, k, across_x, size):
        place = both.at[m, pl.ds(pl.multiple_of(source * local + g * half, 16), size)]
        at = (way * 2 + m) * last + k
        return pltpu.make_async_remote_copy(
            place, place, (xs if across_x else zs).at[at], zr.at[0],
            device_id=(other, f, t) if across_x else hop(way), device_id_type=MESH)

    def arrival(way, m, k, q):
        place = where(m, origin(way, k), g, q)
        return pltpu.make_async_remote_copy(
            place, place, zs.at[0], zr.at[z_at(way, m, k - 1, q)],
            device_id=hop(way), device_id_type=MESH)

    def x_at(way, m, k, q):
        two = k <= double
        base = jnp.where(two, 2 * count * (k - 1), count * (k - 1 + double))
        return m * span + base + jnp.where(two, 2 * q + way, q)

    def x_of(i):
        m, j = lax.div(i, span), lax.rem(i, span)
        two = j < 2 * count * double
        single = jnp.maximum(j - 2 * count * double, 0)
        k = jnp.where(two, 1 + lax.div(j, 2 * count), 1 + double + lax.div(single, count))
        q = jnp.where(two, lax.div(lax.rem(j, 2 * count), 2), lax.rem(single, count))
        up_side = jnp.where(two, lax.rem(j, 2), jnp.where(f < last - f, 1, 0))
        source = f + (2 * up_side - 1) * k
        return m, source, q

    def across(m, source, which, q, sent, i, size=rows):
        first = pl.multiple_of(source * local + which * half + q * rows, 16)
        place = both.at[m, pl.ds(first, size)]
        return pltpu.make_async_remote_copy(
            place, place, xs.at[sent], xr.at[i], device_id=(other, f, t), device_id_type=MESH)

    def send_own(m, q):
        for way in range(2):
            @pl.when(has[way])
            def _(way=way):
                along(way, m, 0, q).start()

    lax.fori_loop(0, slots, lambda i, c: (next_load(i), c)[1], 0)
    token_copy = pltpu.make_async_copy(tokens, held, token_s.at[0])
    token_copy.start()

    barrier = pltpu.get_barrier_semaphore()
    for way in range(2):
        @pl.when(has[way])
        def _(way=way):
            pl.semaphore_signal(barrier, inc=1, device_id=hop(way), device_id_type=MESH)
    pl.semaphore_signal(barrier, inc=1, device_id=(other, f, t), device_id_type=MESH)

    def mate(j):
        return lax.rem(t + j, tp)

    for j in range(1, tp):
        pl.semaphore_signal(barrier, inc=1, device_id=(g, f, mate(j)), device_id_type=MESH)
    step_rows = divisor(local, 128, 8)
    eye = lax.broadcasted_iota(jnp.int32, (step_rows, step_rows), 0) == lax.broadcasted_iota(
        jnp.int32, (step_rows, step_rows), 1)
    for i in range(local // step_rows):
        line = gain[i:i + 1, :]
        column[i * step_rows:(i + 1) * step_rows, :] = jnp.sum(
            jnp.where(eye, line, 0.0), axis=1, keepdims=True)
    pl.semaphore_wait(barrier, tp + jnp.minimum(f, 1) + jnp.minimum(last - f, 1))

    def first_step(q, carry):
        convert(0, g, q, q)

        @pl.when(q > 0)
        def _():
            send_own(0, q - 1)
        return carry

    lax.fori_loop(0, count, first_step, 0)
    token_copy.wait()
    values = held[...].astype(jnp.float32)
    square_mean = jnp.mean(values * values, axis=1, keepdims=True)
    send_own(0, count - 1)
    scaled = (values * lax.rsqrt(square_mean + 1e-06)).astype(jnp.bfloat16)
    for i in range(normed.shape[0]):
        normed[i] = scaled[:, i * block:(i + 1) * block]
    acc[...] = jnp.zeros_like(acc)

    def slot_of(period, slot):
        i = period * per_block - 1
        m, j = lax.div(i, span), lax.rem(i, span)
        k, q = 1 + lax.div(j, count), lax.rem(j, count)
        z_block = g * blocks + lax.div(q, per_block)
        two = j < 2 * count * double
        single = jnp.maximum(j - 2 * count * double, 0)
        xk = jnp.where(two, 1 + lax.div(j, 2 * count), 1 + double + lax.div(single, count))
        xq = jnp.where(two, lax.div(lax.rem(j, 2 * count), 2), lax.rem(single, count))
        x_full = jnp.where(two, lax.rem(j, 2 * per_block) == 2 * per_block - 1, slot == 2)
        above = jnp.where(two, slot == 3, f < last - f)
        source = jnp.where(above, f + xk, f - xk)
        own = lax.div(j + 1 - count, per_block)
        exists = (period > 0) & jnp.where(
            slot == 0, k <= f, jnp.where(
                slot == 1, k <= last - f, jnp.where(
                    slot == 4, (j + 1 >= count) & (own < every), x_full)))
        index = jnp.where(
            slot == 0, (f - k) * every + z_block, jnp.where(
                slot == 1, (f + k) * every + z_block, jnp.where(
                    slot == 4, f * every + own,
                    source * every + other * blocks + lax.div(xq, per_block))))
        return exists, m, index

    def multiply(m, index, slot, p):
        first = pl.multiple_of(index * block, 16)
        at = pl.multiple_of(p * piece, piece)

        @pl.when(m == 0)
        def _():
            acc[p] += jnp.dot(
                normed[index], both[0, pl.ds(first, block), pl.ds(at, piece)],
                preferred_element_type=jnp.float32)

        @pl.when(m == 1)
        def _():
            value = lax.dot_general(
                hidden[p], both[1, pl.ds(first, block), pl.ds(at, piece)],
                (((1,), (1,)), ((), ())), preferred_element_type=jnp.float32)

            @pl.when(p == 0)
            def _():
                product[slot] = value

            @pl.when(p > 0)
            def _():
                product[slot] += value

    def share_out(index, j):
        at = index * (tp - 1) + j - 1
        return pltpu.make_async_remote_copy(
            part.at[index, mate(j)], far.at[index, j - 1], ss.at[j - 1], sr.at[at],
            device_id=(g, f, mate(j)), device_id_type=MESH)

    def stage(which, period, low=0, high=5):
        def one(slot, carry):
            exists, m, index = slot_of(period, slot)

            @pl.when(exists & (m == 1))
            def _():
                if which == 0:
                    for j in range(tp):
                        part[index, j] = product[slot, j * share:(j + 1) * share].astype(jnp.bfloat16)
                elif which == 1:
                    for j in range(1, tp):
                        share_out(index, j).start()
                else:
                    value = part[index, t].astype(jnp.float32)
                    for j in range(1, tp):
                        share_out(index, j).wait_recv()
                        value = value + far[index, j - 1].astype(jnp.float32)
                    out[index] = value.astype(jnp.bfloat16)
            return carry

        lax.fori_loop(low, high, one, 0)

    def chunk_product(source, which, q):
        first = pl.multiple_of(source * local + which * half + q * rows, 16)
        value = jnp.zeros(ending.shape[2:], jnp.float32)
        for p in range(pieces):
            value = value + lax.dot_general(
                hidden[p], both[1, pl.ds(first, rows), p * piece:(p + 1) * piece],
                (((1,), (1,)), ((), ())), preferred_element_type=jnp.float32)
        return value

    def forward(s):
        m, j = lax.div(s, span), lax.rem(s, span)
        k, q = 1 + lax.div(j, count), lax.rem(j, count)

        @pl.when(s < count)
        def _():
            for w in range(2):
                convert(w, other, s, count + 2 * s + w)

        @pl.when((s >= span - count) & (s < span))
        def _():
            convert(1, g, s - (span - count), 3 * count + s - (span - count))

        @pl.when((s > span - count) & (s <= span))
        def _():
            send_own(1, s - 1 - (span - count))

        if extra:
            for way in range(2):
                @pl.when((s == span) & (f == ends[way]))
                def _(way=way):
                    extra_rows(way, f).start()

        for way in range(2):
            @pl.when(reach(way, k))
            def _(way=way):
                arrival(way, m, k, q).wait_recv()

                @pl.when(has[way])
                def _():
                    along(way, m, k, q).start()
                short = shortened(m, origin(way, k), q)
                for size, chosen in ((rows, ~short), (rows - extra, short)):
                    @pl.when(chosen)
                    def _(size=size):
                        across(
                            m, origin(way, k), g, q, (way * 2 + m) * last + k - 1,
                            x_at(way, m, k, q), size).start()

        if extra:
            for way in range(2):
                @pl.when((m == 1) & (q == count - 1) & reach(way, k) & (origin(way, k) == ends[way]) & has[way])
                def _(way=way):
                    extra_rows(way, ends[way]).wait_recv()
                    extra_rows(way, ends[way]).start()

        if single:
            @pl.when((s >= total - per_block) & (reach(0, k) | reach(1, k)))
            def _():
                ending[1, lax.rem(q, per_block)] = chunk_product(last - f, g, q)

    def run(period, low, high, first, end):
        def one(slot, carry):
            exists, m, index = slot_of(period, slot)

            @pl.when(exists)
            def _():
                def body(r, carry):
                    multiply(m, index, slot, r)
                    return carry
                lax.fori_loop(first, end, body, 0)
            return carry

        lax.fori_loop(low, high, one, 0)

    def take(i):
        m = lax.div(i, span)
        _, source, xq = x_of(i)
        short = shortened(m, source, xq)
        for size, chosen in ((rows, ~short), (rows - extra, short)):
            @pl.when(chosen)
            def _(size=size):
                across(0, source, other, xq, 0, i, size).wait_recv()
        return source, xq

    def take_and_multiply(i):
        source, xq = take(i)
        if single:
            @pl.when(i >= total - per_block)
            def _():
                ending[0, lax.rem(i, per_block)] = chunk_product(source, other, xq)

    def absorb(i, low, high, wait):
        if wait:
            take_and_multiply(i)
        rest(i, low, high, wait)

    def rest(i, low, high, wait):
        period, p = lax.div(i, per_block), lax.rem(i, per_block)

        @pl.when(p <= trigger)
        def _():
            run(period, low, high, jnp.minimum(p * each, pieces), jnp.minimum((p + 1) * each, pieces))

        @pl.when(p == trigger)
        def _():
            stage(0, period, low, high)
            stage(1, period, low, high)
            if wait:
                stage(2, period - 1)

        if wait:
            @pl.when(i == span + trigger)
            def _():
                for r in range(pieces):
                    hidden[r] = jnp.square(jnp.maximum(acc[r], 0.0)).astype(jnp.bfloat16)

    def step(s, carry):
        forward(s)

        @pl.when(s >= LAG)
        def _():
            absorb(s - LAG, 0, 5, True)
        return carry

    lax.fori_loop(0, total, step, 0)
    def drain(low, high, wait, end):
        def one(i, carry):
            absorb(i, low, high, wait)
            return carry

        lax.fori_loop(total - LAG, end, one, 0)

    def finish(r, carry):
        m, k = lax.div(r, last), lax.rem(r, last)
        for way in range(2):
            @pl.when(has[way] & ((k == 0) | reach(way, k)))
            def _(way=way):
                all_rows(m, origin(way, k), way, k, False, half).wait_send()

            short = shortened(m, origin(way, k + 1), count - 1)
            for size, chosen in ((half, ~short), (half - extra, short)):
                @pl.when(reach(way, k + 1) & chosen)
                def _(way=way, size=size):
                    all_rows(m, origin(way, k + 1), way, k, True, size).wait_send()
        return carry

    def finish_all():
        lax.fori_loop(0, 2 * last, finish, 0)
        if extra:
            for way in range(2):
                @pl.when(has[way])
                def _(way=way):
                    extra_rows(way, ends[way]).wait_send()

    def take_extra():
        if extra:
            for way in range(2):
                @pl.when(f == ends[1 - way])
                def _(way=way):
                    extra_rows(way, ends[way]).wait_recv()

    def fill(which, index, low, high):
        for p in range(low, high):
            value = ending[which, p].astype(jnp.bfloat16)
            for j in range(tp):
                part[index, j, :, p * rows:(p + 1) * rows] = value[j * share:(j + 1) * share]

    def share_all(index):
        for j in range(1, tp):
            share_out(index, j).start()

    def collect(index):
        value = part[index, t].astype(jnp.float32)
        for j in range(1, tp):
            share_out(index, j).wait_recv()
            value = value + far[index, j - 1].astype(jnp.float32)
        out[index] = value.astype(jnp.bfloat16)

    drain(0, 2, False, total)
    if single:
        far_end = (f == 0) | (f == last)
        z_index = (last - f) * every + g * blocks + blocks - 1

        @pl.when(far_end)
        def _():
            fill(1, z_index, 0, per_block)
            share_all(z_index)

        drain(2, 5, True, total - 1)
        rest(total - 1, 2, 5, True)
        stage(2, final - 1)
        _, source, _ = x_of(total - 1)
        index = source * every + other * blocks + blocks - 1
        fill(0, index, 0, per_block - 1)
        take_extra()
        take(total - 1)
        ending[0, per_block - 1] = chunk_product(source, other, count - 1)
        fill(0, index, per_block - 1, per_block)
        share_all(index)
        finish_all()

        @pl.when(far_end)
        def _():
            collect(z_index)

        collect(index)
    else:
        take_extra()
        drain(2, 5, True, total)
        run(final, 0, 4, 0, pieces)
        stage(0, final, 0, 4)
        stage(1, final, 0, 4)
        finish_all()
        stage(2, final - 1)
        stage(2, final, 0, 4)
    for j in range(1, tp):
        pltpu.make_async_remote_copy(
            part.at[:, mate(j)], far.at[:, j - 1], ss.at[j - 1], sr.at[0],
            device_id=(g, f, mate(j)), device_id_type=MESH).wait_send()


def gather(n, tp, tokens, gain, up, down):
    local, width = up.shape
    count_rows = tokens.shape[0]
    half = local // 2
    block = divisor(half, 256, 16)
    rows = chunk_rows(block, width)
    count = half // rows
    depth = n * local
    piece = next(size for size in (512, 256, 128, width) if width % size == 0)
    moves = 2 * (n - 1) * count
    share, total = count_rows // tp, depth // block
    dma = pltpu.SemaphoreType.DMA
    step_rows = divisor(local, 128, 8)
    sent = 3 * (n - 1) * local * width * 2
    anywhere = pl.BlockSpec(memory_space=pl.ANY)
    inside = pl.BlockSpec(memory_space=pltpu.VMEM)
    return pl.pallas_call(
        functools.partial(gather_kernel, (n, tp, local, block, rows, piece)),
        out_shape=[
            pltpu.VMEM((2, depth, width), jnp.bfloat16),
            pltpu.VMEM((total, share, block), jnp.bfloat16),
        ],
        in_specs=[anywhere, inside, anywhere, anywhere],
        out_specs=[inside, inside],
        scratch_shapes=[
            pltpu.VMEM((min(SLOTS, 4 * count), rows, width), jnp.float32),
            pltpu.VMEM((local, 1), jnp.float32),
            pltpu.VMEM((count_rows, depth), jnp.bfloat16),
            pltpu.VMEM((depth // block, count_rows, block), jnp.bfloat16),
            pltpu.VMEM((width // piece, count_rows, piece), jnp.float32),
            pltpu.VMEM((width // piece, count_rows, piece), jnp.bfloat16),
            pltpu.VMEM((5, count_rows, block), jnp.float32),
            pltpu.VMEM((2, block // rows, count_rows, rows), jnp.float32),
            pltpu.VMEM((total, tp, share, block), jnp.bfloat16),
            pltpu.VMEM((total, tp - 1, share, block), jnp.bfloat16),
            dma((min(SLOTS, 4 * count),)),
            dma((1,)),
            dma((4 * (n - 1),)),
            dma((2 * moves,)),
            dma((4 * (n - 1),)),
            dma((moves,)),
            dma((2,)),
            dma((2,)),
            dma((tp - 1,)),
            dma((total * (tp - 1),)),
        ],
        compiler_params=pltpu.CompilerParams(
            collective_id=0, has_side_effects=True, vmem_limit_bytes=27 * 512 * 1024),
        cost_estimate=pl.CostEstimate(flops=0, bytes_accessed=sent, transcendentals=0),
        name="gather_both",
    )(tokens, gain.reshape(local // step_rows, step_rows), up, down)


def write_kernel(parts, both, mixed, up_ready, down_ready, mixed_out, done):
    depth = both.shape[1]
    size = depth // parts
    copies = []
    for m, ready in enumerate((up_ready, down_ready)):
        for i in range(parts):
            place = pl.ds(i * size, size)
            copies.append(pltpu.make_async_copy(both.at[m, place], ready.at[place], done.at[m * parts + i]))
    for copy in copies:
        copy.start()
    block = mixed.shape[2]
    for i in range(mixed.shape[0]):
        mixed_out[:, i * block:(i + 1) * block] = mixed[i]
    for copy in copies:
        copy.wait()


def per_device(n, tp, tokens, norm_gain, up_master, down_master):
    both, mixed = gather(n, tp, tokens, norm_gain, up_master, down_master)
    depth, width = both.shape[1:]
    share = mixed.shape[1]
    weight = jax.ShapeDtypeStruct((depth, width), jnp.bfloat16)
    anywhere = pl.BlockSpec(memory_space=pl.ANY)
    inside = pl.BlockSpec(memory_space=pltpu.VMEM)
    parts = 8
    return tuple(pl.pallas_call(
        functools.partial(write_kernel, parts),
        out_shape=[weight, weight, jax.ShapeDtypeStruct((share, depth), jnp.bfloat16)],
        in_specs=[anywhere, inside],
        out_specs=[anywhere, anywhere, inside],
        scratch_shapes=[pltpu.SemaphoreType.DMA((2 * parts,))],
        compiler_params=pltpu.CompilerParams(vmem_limit_bytes=27 * 512 * 1024),
        name="write_out",
    )(pltpu.with_memory_space_constraint(both, pltpu.VMEM), pltpu.with_memory_space_constraint(mixed, pltpu.VMEM)))


def solution(mesh):
    n, tp = (mesh.shape[name] for name in ("fs", "tp"))
    return jax.shard_map(
        functools.partial(per_device, n, tp),
        mesh=mesh,
        in_specs=(P(("grp", "fs"), None), P("fs"), P("fs", "tp"), P("fs", "tp")),
        out_specs=(P("grp", "tp"), P("grp", "tp"), P(("grp", "fs", "tp"), None)),
        check_vma=False,
    )
```

```python
import functools

import jax
import jax.numpy as jnp
from jax import lax
from jax.experimental import pallas as pl
from jax.experimental.pallas import tpu as pltpu
from jax.sharding import PartitionSpec as P

MESH = pl.DeviceIdType.MESH
SLOTS = 6
LAG = 1


def divisor(total, most, least):
    for size in range(most, 0, -least):
        if total % size == 0:
            return size
    return total


def chunk_rows(block, width):
    for rows in range(16, block + 1, 16):
        if block % rows == 0 and rows * width * 2 >= 200 * 1024:
            return rows
    return block


def gather_kernel(sizes, tokens, gain, up, down, both, out, wide, column, held, normed, acc, hidden, product,
                  ending, part, far, load, token_s, zs, zr, xs, xr, es, er, ss, sr):
    n, tp, local, block, rows, piece = sizes
    half = local // 2
    count = half // rows
    per_block = block // rows
    blocks = half // block
    last = n - 1
    span = last * count
    total = 2 * span
    slots = wide.shape[0]
    g, f, t = lax.axis_index("grp"), lax.axis_index("fs"), lax.axis_index("tp")
    other = 1 - g
    every = 2 * blocks
    share = part.shape[2]
    final = total // per_block
    extra = rows // 32 * 16
    pieces = acc.shape[0]
    trigger = per_block - 1 - LAG if per_block > 2 * LAG else per_block - 1
    each = -(-pieces // (trigger + 1))
    single = n % 2 == 0
    double = jnp.minimum(f, last - f)

    def start_load(m, which, q, index):
        first = pl.multiple_of(which * half + q * rows, 16)
        slot = lax.rem(index, slots)
        pltpu.make_async_copy((up, down)[m].at[pl.ds(first, rows)], wide.at[slot], load.at[slot]).start()

    def next_load(index):
        @pl.when(index < count)
        def _():
            start_load(0, g, index, index)

        for m in range(2):
            @pl.when((index >= count) & (index < 3 * count) & (lax.rem(index + count, 2) == m))
            def _(m=m):
                start_load(m, other, lax.div(index - count, 2), index)

        @pl.when((index >= 3 * count) & (index < 4 * count))
        def _():
            start_load(1, g, index - 3 * count, index)

    def where(m, source, which, q):
        first = pl.multiple_of(source * local + which * half + q * rows, 16)
        return both.at[m, pl.ds(first, rows)]

    def convert(m, which, q, index):
        slot = lax.rem(index, slots)
        pltpu.make_async_copy(up.at[pl.ds(0, rows)], wide.at[slot], load.at[slot]).wait()
        near = pl.multiple_of(which * half + q * rows, 16)
        first = pl.multiple_of(f * local + which * half + q * rows, 16)
        values = wide[slot]
        if m == 0:
            values = column[pl.ds(near, rows)] * values
        both[m, pl.ds(first, rows)] = values.astype(jnp.bfloat16)
        next_load(index + slots)

    has = (f < last, f > 0)

    def hop(way):
        return (g, f + 1 if way == 0 else f - 1, t)

    def origin(way, k):
        return f - k if way == 0 else f + k

    def reach(way, k):
        return (k <= f) if way == 0 else (k <= last - f)

    def z_at(way, m, k, q):
        return ((way * 2 + m) * last + k) * count + q

    def along(way, m, k, q):
        place = where(m, origin(way, k), g, q)
        return pltpu.make_async_remote_copy(
            place, place, zs.at[(way * 2 + m) * last + k], zr.at[z_at(way, m, k, q)],
            device_id=hop(way), device_id_type=MESH)

    ends = (0, last)

    def shortened(m, source, q):
        return (m == 1) & (q == count - 1) & ((source == 0) | (source == last)) & (extra > 0)

    def extra_rows(way, source):
        first = pl.multiple_of(source * local + other * half + half - extra, 16)
        place = both.at[1, pl.ds(first, extra)]
        return pltpu.make_async_remote_copy(
            place, place, es.at[way], er.at[way], device_id=hop(way), device_id_type=MESH)

    def all_rows(m, source, way, k, across_x, size):
        place = both.at[m, pl.ds(pl.multiple_of(source * local + g * half, 16), size)]
        at = (way * 2 + m) * last + k
        return pltpu.make_async_remote_copy(
            place, place, (xs if across_x else zs).at[at], zr.at[0],
            device_id=(other, f, t) if across_x else hop(way), device_id_type=MESH)

    def arrival(way, m, k, q):
        place = where(m, origin(way, k), g, q)
        return pltpu.make_async_remote_copy(
            place, place, zs.at[0], zr.at[z_at(way, m, k - 1, q)],
            device_id=hop(way), device_id_type=MESH)

    def x_at(way, m, k, q):
        two = k <= double
        base = jnp.where(two, 2 * count * (k - 1), count * (k - 1 + double))
        return m * span + base + jnp.where(two, 2 * q + way, q)

    def x_of(i):
        m, j = lax.div(i, span), lax.rem(i, span)
        two = j < 2 * count * double
        single = jnp.maximum(j - 2 * count * double, 0)
        k = jnp.where(two, 1 + lax.div(j, 2 * count), 1 + double + lax.div(single, count))
        q = jnp.where(two, lax.div(lax.rem(j, 2 * count), 2), lax.rem(single, count))
        up_side = jnp.where(two, lax.rem(j, 2), jnp.where(f < last - f, 1, 0))
        source = f + (2 * up_side - 1) * k
        return m, source, q

    def across(m, source, which, q, sent, i, size=rows):
        first = pl.multiple_of(source * local + which * half + q * rows, 16)
        place = both.at[m, pl.ds(first, size)]
        return pltpu.make_async_remote_copy(
            place, place, xs.at[sent], xr.at[i], device_id=(other, f, t), device_id_type=MESH)

    def send_own(m, q):
        for way in range(2):
            @pl.when(has[way])
            def _(way=way):
                along(way, m, 0, q).start()

    lax.fori_loop(0, slots, lambda i, c: (next_load(i), c)[1], 0)
    token_copy = pltpu.make_async_copy(tokens, held, token_s.at[0])
    token_copy.start()

    barrier = pltpu.get_barrier_semaphore()
    for way in range(2):
        @pl.when(has[way])
        def _(way=way):
            pl.semaphore_signal(barrier, inc=1, device_id=hop(way), device_id_type=MESH)
    pl.semaphore_signal(barrier, inc=1, device_id=(other, f, t), device_id_type=MESH)

    def mate(j):
        return lax.rem(t + j, tp)

    for j in range(1, tp):
        pl.semaphore_signal(barrier, inc=1, device_id=(g, f, mate(j)), device_id_type=MESH)
    step_rows = divisor(local, 128, 8)
    eye = lax.broadcasted_iota(jnp.int32, (step_rows, step_rows), 0) == lax.broadcasted_iota(
        jnp.int32, (step_rows, step_rows), 1)
    for i in range(local // step_rows):
        line = gain[i:i + 1, :]
        column[i * step_rows:(i + 1) * step_rows, :] = jnp.sum(
            jnp.where(eye, line, 0.0), axis=1, keepdims=True)
    pl.semaphore_wait(barrier, tp + jnp.minimum(f, 1) + jnp.minimum(last - f, 1))

    def first_step(q, carry):
        convert(0, g, q, q)

        @pl.when(q > 0)
        def _():
            send_own(0, q - 1)
        return carry

    lax.fori_loop(0, count, first_step, 0)
    token_copy.wait()
    values = held[...].astype(jnp.float32)
    square_mean = jnp.mean(values * values, axis=1, keepdims=True)
    send_own(0, count - 1)
    scaled = (values * lax.rsqrt(square_mean + 1e-06)).astype(jnp.bfloat16)
    for i in range(normed.shape[0]):
        normed[i] = scaled[:, i * block:(i + 1) * block]
    acc[...] = jnp.zeros_like(acc)

    def slot_of(period, slot):
        i = period * per_block - 1
        m, j = lax.div(i, span), lax.rem(i, span)
        k, q = 1 + lax.div(j, count), lax.rem(j, count)
        z_block = g * blocks + lax.div(q, per_block)
        two = j < 2 * count * double
        single = jnp.maximum(j - 2 * count * double, 0)
        xk = jnp.where(two, 1 + lax.div(j, 2 * count), 1 + double + lax.div(single, count))
        xq = jnp.where(two, lax.div(lax.rem(j, 2 * count), 2), lax.rem(single, count))
        x_full = jnp.where(two, lax.rem(j, 2 * per_block) == 2 * per_block - 1, slot == 2)
        above = jnp.where(two, slot == 3, f < last - f)
        source = jnp.where(above, f + xk, f - xk)
        own = lax.div(j + 1 - count, per_block)
        exists = (period > 0) & jnp.where(
            slot == 0, k <= f, jnp.where(
                slot == 1, k <= last - f, jnp.where(
                    slot == 4, (j + 1 >= count) & (own < every), x_full)))
        index = jnp.where(
            slot == 0, (f - k) * every + z_block, jnp.where(
                slot == 1, (f + k) * every + z_block, jnp.where(
                    slot == 4, f * every + own,
                    source * every + other * blocks + lax.div(xq, per_block))))
        return exists, m, index

    def multiply(m, index, slot, p):
        first = pl.multiple_of(index * block, 16)
        at = pl.multiple_of(p * piece, piece)

        @pl.when(m == 0)
        def _():
            acc[p] += jnp.dot(
                normed[index], both[0, pl.ds(first, block), pl.ds(at, piece)],
                preferred_element_type=jnp.float32)

        @pl.when(m == 1)
        def _():
            value = lax.dot_general(
                hidden[p], both[1, pl.ds(first, block), pl.ds(at, piece)],
                (((1,), (1,)), ((), ())), preferred_element_type=jnp.float32)

            @pl.when(p == 0)
            def _():
                product[slot] = value

            @pl.when(p > 0)
            def _():
                product[slot] += value

    def share_out(index, j):
        at = index * (tp - 1) + j - 1
        return pltpu.make_async_remote_copy(
            part.at[index, mate(j)], far.at[index, j - 1], ss.at[j - 1], sr.at[at],
            device_id=(g, f, mate(j)), device_id_type=MESH)

    def stage(which, period, low=0, high=5):
        def one(slot, carry):
            exists, m, index = slot_of(period, slot)

            @pl.when(exists & (m == 1))
            def _():
                if which == 0:
                    for j in range(tp):
                        part[index, j] = product[slot, j * share:(j + 1) * share].astype(jnp.bfloat16)
                elif which == 1:
                    for j in range(1, tp):
                        share_out(index, j).start()
                else:
                    value = part[index, t].astype(jnp.float32)
                    for j in range(1, tp):
                        share_out(index, j).wait_recv()
                        value = value + far[index, j - 1].astype(jnp.float32)
                    out[index] = value.astype(jnp.bfloat16)
            return carry

        lax.fori_loop(low, high, one, 0)

    def chunk_product(source, which, q):
        first = pl.multiple_of(source * local + which * half + q * rows, 16)
        value = jnp.zeros(ending.shape[2:], jnp.float32)
        for p in range(pieces):
            value = value + lax.dot_general(
                hidden[p], both[1, pl.ds(first, rows), p * piece:(p + 1) * piece],
                (((1,), (1,)), ((), ())), preferred_element_type=jnp.float32)
        return value

    def forward(s):
        m, j = lax.div(s, span), lax.rem(s, span)
        k, q = 1 + lax.div(j, count), lax.rem(j, count)

        @pl.when(s < count)
        def _():
            for w in range(2):
                convert(w, other, s, count + 2 * s + w)

        @pl.when((s >= span - count) & (s < span))
        def _():
            convert(1, g, s - (span - count), 3 * count + s - (span - count))

        @pl.when((s > span - count) & (s <= span))
        def _():
            send_own(1, s - 1 - (span - count))

        if extra:
            for way in range(2):
                @pl.when((s == span) & (f == ends[way]))
                def _(way=way):
                    extra_rows(way, f).start()

        for way in range(2):
            @pl.when(reach(way, k))
            def _(way=way):
                arrival(way, m, k, q).wait_recv()

                @pl.when(has[way])
                def _():
                    along(way, m, k, q).start()
                short = shortened(m, origin(way, k), q)
                for size, chosen in ((rows, ~short), (rows - extra, short)):
                    @pl.when(chosen)
                    def _(size=size):
                        across(
                            m, origin(way, k), g, q, (way * 2 + m) * last + k - 1,
                            x_at(way, m, k, q), size).start()

        if extra:
            for way in range(2):
                @pl.when((m == 1) & (q == count - 1) & reach(way, k) & (origin(way, k) == ends[way]) & has[way])
                def _(way=way):
                    extra_rows(way, ends[way]).wait_recv()
                    extra_rows(way, ends[way]).start()

        if single:
            @pl.when((s >= total - per_block) & (reach(0, k) | reach(1, k)))
            def _():
                ending[1, lax.rem(q, per_block)] = chunk_product(last - f, g, q)

    def run(period, low, high, first, end):
        def one(slot, carry):
            exists, m, index = slot_of(period, slot)

            @pl.when(exists)
            def _():
                def body(r, carry):
                    multiply(m, index, slot, r)
                    return carry
                lax.fori_loop(first, end, body, 0)
            return carry

        lax.fori_loop(low, high, one, 0)

    def take(i):
        m = lax.div(i, span)
        _, source, xq = x_of(i)
        short = shortened(m, source, xq)
        for size, chosen in ((rows, ~short), (rows - extra, short)):
            @pl.when(chosen)
            def _(size=size):
                across(0, source, other, xq, 0, i, size).wait_recv()
        return source, xq

    def take_and_multiply(i):
        source, xq = take(i)
        if single:
            @pl.when(i >= total - per_block)
            def _():
                ending[0, lax.rem(i, per_block)] = chunk_product(source, other, xq)

    def absorb(i, low, high, wait):
        if wait:
            take_and_multiply(i)
        rest(i, low, high, wait)

    def rest(i, low, high, wait):
        period, p = lax.div(i, per_block), lax.rem(i, per_block)

        @pl.when(p <= trigger)
        def _():
            run(period, low, high, jnp.minimum(p * each, pieces), jnp.minimum((p + 1) * each, pieces))

        @pl.when(p == trigger)
        def _():
            stage(0, period, low, high)
            stage(1, period, low, high)
            if wait:
                stage(2, period - 1)

        if wait:
            @pl.when(i == span + trigger)
            def _():
                for r in range(pieces):
                    hidden[r] = jnp.square(jnp.maximum(acc[r], 0.0)).astype(jnp.bfloat16)

    def step(s, carry):
        forward(s)

        @pl.when(s >= LAG)
        def _():
            absorb(s - LAG, 0, 5, True)
        return carry

    lax.fori_loop(0, total, step, 0)
    def drain(low, high, wait, end):
        def one(i, carry):
            absorb(i, low, high, wait)
            return carry

        lax.fori_loop(total - LAG, end, one, 0)

    def finish(r, carry):
        m, k = lax.div(r, last), lax.rem(r, last)
        for way in range(2):
            @pl.when(has[way] & ((k == 0) | reach(way, k)))
            def _(way=way):
                all_rows(m, origin(way, k), way, k, False, half).wait_send()

            short = shortened(m, origin(way, k + 1), count - 1)
            for size, chosen in ((half, ~short), (half - extra, short)):
                @pl.when(reach(way, k + 1) & chosen)
                def _(way=way, size=size):
                    all_rows(m, origin(way, k + 1), way, k, True, size).wait_send()
        return carry

    def finish_all():
        lax.fori_loop(0, 2 * last, finish, 0)
        if extra:
            for way in range(2):
                @pl.when(has[way])
                def _(way=way):
                    extra_rows(way, ends[way]).wait_send()

    def take_extra():
        if extra:
            for way in range(2):
                @pl.when(f == ends[1 - way])
                def _(way=way):
                    extra_rows(way, ends[way]).wait_recv()

    def fill(which, index, low, high):
        for p in range(low, high):
            value = ending[which, p].astype(jnp.bfloat16)
            for j in range(tp):
                part[index, j, :, p * rows:(p + 1) * rows] = value[j * share:(j + 1) * share]

    def share_all(index):
        for j in range(1, tp):
            share_out(index, j).start()

    def collect(index):
        value = part[index, t].astype(jnp.float32)
        for j in range(1, tp):
            share_out(index, j).wait_recv()
            value = value + far[index, j - 1].astype(jnp.float32)
        out[index] = value.astype(jnp.bfloat16)

    drain(0, 2, False, total)
    if single:
        far_end = (f == 0) | (f == last)
        z_index = (last - f) * every + g * blocks + blocks - 1

        @pl.when(far_end)
        def _():
            fill(1, z_index, 0, per_block)
            share_all(z_index)

        drain(2, 5, True, total - 1)
        rest(total - 1, 2, 5, True)
        _, source, _ = x_of(total - 1)
        index = source * every + other * blocks + blocks - 1
        fill(0, index, 0, per_block - 1)
        take_extra()
        take(total - 1)
        ending[0, per_block - 1] = chunk_product(source, other, count - 1)
        fill(0, index, per_block - 1, per_block)
        share_all(index)
        finish_all()
        stage(2, final - 1)

        @pl.when(far_end)
        def _():
            collect(z_index)

        collect(index)
    else:
        take_extra()
        drain(2, 5, True, total)
        run(final, 0, 4, 0, pieces)
        stage(0, final, 0, 4)
        stage(1, final, 0, 4)
        finish_all()
        stage(2, final - 1)
        stage(2, final, 0, 4)
    for j in range(1, tp):
        pltpu.make_async_remote_copy(
            part.at[:, mate(j)], far.at[:, j - 1], ss.at[j - 1], sr.at[0],
            device_id=(g, f, mate(j)), device_id_type=MESH).wait_send()


def gather(n, tp, tokens, gain, up, down):
    local, width = up.shape
    count_rows = tokens.shape[0]
    half = local // 2
    block = divisor(half, 256, 16)
    rows = chunk_rows(block, width)
    count = half // rows
    depth = n * local
    piece = next(size for size in (512, 256, 128, width) if width % size == 0)
    moves = 2 * (n - 1) * count
    share, total = count_rows // tp, depth // block
    dma = pltpu.SemaphoreType.DMA
    step_rows = divisor(local, 128, 8)
    sent = 3 * (n - 1) * local * width * 2
    anywhere = pl.BlockSpec(memory_space=pl.ANY)
    inside = pl.BlockSpec(memory_space=pltpu.VMEM)
    return pl.pallas_call(
        functools.partial(gather_kernel, (n, tp, local, block, rows, piece)),
        out_shape=[
            pltpu.VMEM((2, depth, width), jnp.bfloat16),
            pltpu.VMEM((total, share, block), jnp.bfloat16),
        ],
        in_specs=[anywhere, inside, anywhere, anywhere],
        out_specs=[inside, inside],
        scratch_shapes=[
            pltpu.VMEM((min(SLOTS, 4 * count), rows, width), jnp.float32),
            pltpu.VMEM((local, 1), jnp.float32),
            pltpu.VMEM((count_rows, depth), jnp.bfloat16),
            pltpu.VMEM((depth // block, count_rows, block), jnp.bfloat16),
            pltpu.VMEM((width // piece, count_rows, piece), jnp.float32),
            pltpu.VMEM((width // piece, count_rows, piece), jnp.bfloat16),
            pltpu.VMEM((5, count_rows, block), jnp.float32),
            pltpu.VMEM((2, block // rows, count_rows, rows), jnp.float32),
            pltpu.VMEM((total, tp, share, block), jnp.bfloat16),
            pltpu.VMEM((total, tp - 1, share, block), jnp.bfloat16),
            dma((min(SLOTS, 4 * count),)),
            dma((1,)),
            dma((4 * (n - 1),)),
            dma((2 * moves,)),
            dma((4 * (n - 1),)),
            dma((moves,)),
            dma((2,)),
            dma((2,)),
            dma((tp - 1,)),
            dma((total * (tp - 1),)),
        ],
        compiler_params=pltpu.CompilerParams(
            collective_id=0, has_side_effects=True, vmem_limit_bytes=27 * 512 * 1024),
        cost_estimate=pl.CostEstimate(flops=0, bytes_accessed=sent, transcendentals=0),
        name="gather_both",
    )(tokens, gain.reshape(local // step_rows, step_rows), up, down)


def write_kernel(parts, both, mixed, up_ready, down_ready, mixed_out, done):
    depth = both.shape[1]
    size = depth // parts
    copies = []
    for m, ready in enumerate((up_ready, down_ready)):
        for i in range(parts):
            place = pl.ds(i * size, size)
            copies.append(pltpu.make_async_copy(both.at[m, place], ready.at[place], done.at[m * parts + i]))
    for copy in copies:
        copy.start()
    block = mixed.shape[2]
    for i in range(mixed.shape[0]):
        mixed_out[:, i * block:(i + 1) * block] = mixed[i]
    for copy in copies:
        copy.wait()


def per_device(n, tp, tokens, norm_gain, up_master, down_master):
    both, mixed = gather(n, tp, tokens, norm_gain, up_master, down_master)
    depth, width = both.shape[1:]
    share = mixed.shape[1]
    weight = jax.ShapeDtypeStruct((depth, width), jnp.bfloat16)
    anywhere = pl.BlockSpec(memory_space=pl.ANY)
    inside = pl.BlockSpec(memory_space=pltpu.VMEM)
    parts = 8
    return tuple(pl.pallas_call(
        functools.partial(write_kernel, parts),
        out_shape=[weight, weight, jax.ShapeDtypeStruct((share, depth), jnp.bfloat16)],
        in_specs=[anywhere, inside],
        out_specs=[anywhere, anywhere, inside],
        scratch_shapes=[pltpu.SemaphoreType.DMA((2 * parts,))],
        compiler_params=pltpu.CompilerParams(vmem_limit_bytes=27 * 512 * 1024),
        name="write_out",
    )(pltpu.with_memory_space_constraint(both, pltpu.VMEM), pltpu.with_memory_space_constraint(mixed, pltpu.VMEM)))


def solution(mesh):
    n, tp = (mesh.shape[name] for name in ("fs", "tp"))
    return jax.shard_map(
        functools.partial(per_device, n, tp),
        mesh=mesh,
        in_specs=(P(("grp", "fs"), None), P("fs"), P("fs", "tp"), P("fs", "tp")),
        out_specs=(P("grp", "tp"), P("grp", "tp"), P(("grp", "fs", "tp"), None)),
        check_vma=False,
    )
```

```python
import functools

import jax
import jax.numpy as jnp
from jax import lax
from jax.experimental import pallas as pl
from jax.experimental.pallas import tpu as pltpu
from jax.sharding import PartitionSpec as P

MESH = pl.DeviceIdType.MESH
SLOTS = 6
LAG = 1


def divisor(total, most, least):
    for size in range(most, 0, -least):
        if total % size == 0:
            return size
    return total


def chunk_rows(block, width):
    for rows in range(16, block + 1, 16):
        if block % rows == 0 and rows * width * 2 >= 200 * 1024:
            return rows
    return block


def gather_kernel(sizes, tokens, gain, up, down, both, out, wide, column, held, normed, acc, hidden, product,
                  ending, part, far, load, token_s, zs, zr, xs, xr, es, er, ss, sr):
    n, tp, local, block, rows, piece = sizes
    half = local // 2
    count = half // rows
    per_block = block // rows
    blocks = half // block
    last = n - 1
    span = last * count
    total = 2 * span
    slots = wide.shape[0]
    g, f, t = lax.axis_index("grp"), lax.axis_index("fs"), lax.axis_index("tp")
    other = 1 - g
    every = 2 * blocks
    share = part.shape[2]
    final = total // per_block
    extra = rows // 32 * 16
    pieces = acc.shape[0]
    trigger = per_block - 1 - LAG if per_block > 2 * LAG else per_block - 1
    each = -(-pieces // (trigger + 1))
    single = n % 2 == 0
    double = jnp.minimum(f, last - f)

    def start_load(m, which, q, index):
        first = pl.multiple_of(which * half + q * rows, 16)
        slot = lax.rem(index, slots)
        pltpu.make_async_copy((up, down)[m].at[pl.ds(first, rows)], wide.at[slot], load.at[slot]).start()

    def next_load(index):
        @pl.when(index < count)
        def _():
            start_load(0, g, index, index)

        for m in range(2):
            @pl.when((index >= count) & (index < 3 * count) & (lax.rem(index + count, 2) == m))
            def _(m=m):
                start_load(m, other, lax.div(index - count, 2), index)

        @pl.when((index >= 3 * count) & (index < 4 * count))
        def _():
            start_load(1, g, index - 3 * count, index)

    def where(m, source, which, q):
        first = pl.multiple_of(source * local + which * half + q * rows, 16)
        return both.at[m, pl.ds(first, rows)]

    def convert(m, which, q, index):
        slot = lax.rem(index, slots)
        pltpu.make_async_copy(up.at[pl.ds(0, rows)], wide.at[slot], load.at[slot]).wait()
        near = pl.multiple_of(which * half + q * rows, 16)
        first = pl.multiple_of(f * local + which * half + q * rows, 16)
        values = wide[slot]
        if m == 0:
            values = column[pl.ds(near, rows)] * values
        both[m, pl.ds(first, rows)] = values.astype(jnp.bfloat16)
        next_load(index + slots)

    has = (f < last, f > 0)

    def hop(way):
        return (g, f + 1 if way == 0 else f - 1, t)

    def origin(way, k):
        return f - k if way == 0 else f + k

    def reach(way, k):
        return (k <= f) if way == 0 else (k <= last - f)

    def z_at(way, m, k, q):
        return ((way * 2 + m) * last + k) * count + q

    def along(way, m, k, q):
        place = where(m, origin(way, k), g, q)
        return pltpu.make_async_remote_copy(
            place, place, zs.at[(way * 2 + m) * last + k], zr.at[z_at(way, m, k, q)],
            device_id=hop(way), device_id_type=MESH)

    ends = (0, last)

    def shortened(m, source, q):
        return (m == 1) & (q == count - 1) & ((source == 0) | (source == last)) & (extra > 0)

    def extra_rows(way, source):
        first = pl.multiple_of(source * local + other * half + half - extra, 16)
        place = both.at[1, pl.ds(first, extra)]
        return pltpu.make_async_remote_copy(
            place, place, es.at[way], er.at[way], device_id=hop(way), device_id_type=MESH)

    def all_rows(m, source, way, k, across_x, size):
        place = both.at[m, pl.ds(pl.multiple_of(source * local + g * half, 16), size)]
        at = (way * 2 + m) * last + k
        return pltpu.make_async_remote_copy(
            place, place, (xs if across_x else zs).at[at], zr.at[0],
            device_id=(other, f, t) if across_x else hop(way), device_id_type=MESH)

    def arrival(way, m, k, q):
        place = where(m, origin(way, k), g, q)
        return pltpu.make_async_remote_copy(
            place, place, zs.at[0], zr.at[z_at(way, m, k - 1, q)],
            device_id=hop(way), device_id_type=MESH)

    def x_at(way, m, k, q):
        two = k <= double
        base = jnp.where(two, 2 * count * (k - 1), count * (k - 1 + double))
        return m * span + base + jnp.where(two, 2 * q + way, q)

    def x_of(i):
        m, j = lax.div(i, span), lax.rem(i, span)
        two = j < 2 * count * double
        single = jnp.maximum(j - 2 * count * double, 0)
        k = jnp.where(two, 1 + lax.div(j, 2 * count), 1 + double + lax.div(single, count))
        q = jnp.where(two, lax.div(lax.rem(j, 2 * count), 2), lax.rem(single, count))
        up_side = jnp.where(two, lax.rem(j, 2), jnp.where(f < last - f, 1, 0))
        source = f + (2 * up_side - 1) * k
        return m, source, q

    def across(m, source, which, q, sent, i, size=rows):
        first = pl.multiple_of(source * local + which * half + q * rows, 16)
        place = both.at[m, pl.ds(first, size)]
        return pltpu.make_async_remote_copy(
            place, place, xs.at[sent], xr.at[i], device_id=(other, f, t), device_id_type=MESH)

    def send_own(m, q):
        for way in range(2):
            @pl.when(has[way])
            def _(way=way):
                along(way, m, 0, q).start()

    start_load(0, g, 0, 0)

    barrier = pltpu.get_barrier_semaphore()
    for way in range(2):
        @pl.when(has[way])
        def _(way=way):
            pl.semaphore_signal(barrier, inc=1, device_id=hop(way), device_id_type=MESH)
    pl.semaphore_signal(barrier, inc=1, device_id=(other, f, t), device_id_type=MESH)

    def mate(j):
        return lax.rem(t + j, tp)

    for j in range(1, tp):
        pl.semaphore_signal(barrier, inc=1, device_id=(g, f, mate(j)), device_id_type=MESH)
    lax.fori_loop(1, slots, lambda i, c: (next_load(i), c)[1], 0)
    token_copy = pltpu.make_async_copy(tokens, held, token_s.at[0])
    token_copy.start()
    step_rows = divisor(local, 128, 8)
    eye = lax.broadcasted_iota(jnp.int32, (step_rows, step_rows), 0) == lax.broadcasted_iota(
        jnp.int32, (step_rows, step_rows), 1)
    for i in range(local // step_rows):
        line = gain[i:i + 1, :]
        column[i * step_rows:(i + 1) * step_rows, :] = jnp.sum(
            jnp.where(eye, line, 0.0), axis=1, keepdims=True)
    pl.semaphore_wait(barrier, tp + jnp.minimum(f, 1) + jnp.minimum(last - f, 1))

    def first_step(q, carry):
        convert(0, g, q, q)

        @pl.when(q > 0)
        def _():
            send_own(0, q - 1)
        return carry

    lax.fori_loop(0, count, first_step, 0)
    token_copy.wait()
    values = held[...].astype(jnp.float32)
    square_mean = jnp.mean(values * values, axis=1, keepdims=True)
    send_own(0, count - 1)
    scaled = (values * lax.rsqrt(square_mean + 1e-06)).astype(jnp.bfloat16)
    for i in range(normed.shape[0]):
        normed[i] = scaled[:, i * block:(i + 1) * block]
    acc[...] = jnp.zeros_like(acc)

    def slot_of(period, slot):
        i = period * per_block - 1
        m, j = lax.div(i, span), lax.rem(i, span)
        k, q = 1 + lax.div(j, count), lax.rem(j, count)
        z_block = g * blocks + lax.div(q, per_block)
        two = j < 2 * count * double
        single = jnp.maximum(j - 2 * count * double, 0)
        xk = jnp.where(two, 1 + lax.div(j, 2 * count), 1 + double + lax.div(single, count))
        xq = jnp.where(two, lax.div(lax.rem(j, 2 * count), 2), lax.rem(single, count))
        x_full = jnp.where(two, lax.rem(j, 2 * per_block) == 2 * per_block - 1, slot == 2)
        above = jnp.where(two, slot == 3, f < last - f)
        source = jnp.where(above, f + xk, f - xk)
        own = lax.div(j + 1 - count, per_block)
        exists = (period > 0) & jnp.where(
            slot == 0, k <= f, jnp.where(
                slot == 1, k <= last - f, jnp.where(
                    slot == 4, (j + 1 >= count) & (own < every), x_full)))
        index = jnp.where(
            slot == 0, (f - k) * every + z_block, jnp.where(
                slot == 1, (f + k) * every + z_block, jnp.where(
                    slot == 4, f * every + own,
                    source * every + other * blocks + lax.div(xq, per_block))))
        return exists, m, index

    def multiply(m, index, slot, p):
        first = pl.multiple_of(index * block, 16)
        at = pl.multiple_of(p * piece, piece)

        @pl.when(m == 0)
        def _():
            acc[p] += jnp.dot(
                normed[index], both[0, pl.ds(first, block), pl.ds(at, piece)],
                preferred_element_type=jnp.float32)

        @pl.when(m == 1)
        def _():
            value = lax.dot_general(
                hidden[p], both[1, pl.ds(first, block), pl.ds(at, piece)],
                (((1,), (1,)), ((), ())), preferred_element_type=jnp.float32)

            @pl.when(p == 0)
            def _():
                product[slot] = value

            @pl.when(p > 0)
            def _():
                product[slot] += value

    def share_out(index, j):
        at = index * (tp - 1) + j - 1
        return pltpu.make_async_remote_copy(
            part.at[index, mate(j)], far.at[index, j - 1], ss.at[j - 1], sr.at[at],
            device_id=(g, f, mate(j)), device_id_type=MESH)

    def stage(which, period, low=0, high=5):
        def one(slot, carry):
            exists, m, index = slot_of(period, slot)

            @pl.when(exists & (m == 1))
            def _():
                if which == 0:
                    for j in range(tp):
                        part[index, j] = product[slot, j * share:(j + 1) * share].astype(jnp.bfloat16)
                elif which == 1:
                    for j in range(1, tp):
                        share_out(index, j).start()
                else:
                    value = part[index, t].astype(jnp.float32)
                    for j in range(1, tp):
                        share_out(index, j).wait_recv()
                        value = value + far[index, j - 1].astype(jnp.float32)
                    out[index] = value.astype(jnp.bfloat16)
            return carry

        lax.fori_loop(low, high, one, 0)

    def chunk_product(source, which, q):
        first = pl.multiple_of(source * local + which * half + q * rows, 16)
        value = jnp.zeros(ending.shape[2:], jnp.float32)
        for p in range(pieces):
            value = value + lax.dot_general(
                hidden[p], both[1, pl.ds(first, rows), p * piece:(p + 1) * piece],
                (((1,), (1,)), ((), ())), preferred_element_type=jnp.float32)
        return value

    def forward(s):
        m, j = lax.div(s, span), lax.rem(s, span)
        k, q = 1 + lax.div(j, count), lax.rem(j, count)

        @pl.when(s < count)
        def _():
            for w in range(2):
                convert(w, other, s, count + 2 * s + w)

        @pl.when((s >= span - count) & (s < span))
        def _():
            convert(1, g, s - (span - count), 3 * count + s - (span - count))

        @pl.when((s > span - count) & (s <= span))
        def _():
            send_own(1, s - 1 - (span - count))

        if extra:
            for way in range(2):
                @pl.when((s == span) & (f == ends[way]))
                def _(way=way):
                    extra_rows(way, f).start()

        for way in range(2):
            @pl.when(reach(way, k))
            def _(way=way):
                arrival(way, m, k, q).wait_recv()

                @pl.when(has[way])
                def _():
                    along(way, m, k, q).start()
                short = shortened(m, origin(way, k), q)
                for size, chosen in ((rows, ~short), (rows - extra, short)):
                    @pl.when(chosen)
                    def _(size=size):
                        across(
                            m, origin(way, k), g, q, (way * 2 + m) * last + k - 1,
                            x_at(way, m, k, q), size).start()

        if extra:
            for way in range(2):
                @pl.when((m == 1) & (q == count - 1) & reach(way, k) & (origin(way, k) == ends[way]) & has[way])
                def _(way=way):
                    extra_rows(way, ends[way]).wait_recv()
                    extra_rows(way, ends[way]).start()

        if single:
            @pl.when((s >= total - per_block) & (reach(0, k) | reach(1, k)))
            def _():
                ending[1, lax.rem(q, per_block)] = chunk_product(last - f, g, q)

    def run(period, low, high, first, end):
        def one(slot, carry):
            exists, m, index = slot_of(period, slot)

            @pl.when(exists)
            def _():
                def body(r, carry):
                    multiply(m, index, slot, r)
                    return carry
                lax.fori_loop(first, end, body, 0)
            return carry

        lax.fori_loop(low, high, one, 0)

    def take(i):
        m = lax.div(i, span)
        _, source, xq = x_of(i)
        short = shortened(m, source, xq)
        for size, chosen in ((rows, ~short), (rows - extra, short)):
            @pl.when(chosen)
            def _(size=size):
                across(0, source, other, xq, 0, i, size).wait_recv()
        return source, xq

    def take_and_multiply(i):
        source, xq = take(i)
        if single:
            @pl.when(i >= total - per_block)
            def _():
                ending[0, lax.rem(i, per_block)] = chunk_product(source, other, xq)

    def absorb(i, low, high, wait):
        if wait:
            take_and_multiply(i)
        rest(i, low, high, wait)

    def rest(i, low, high, wait):
        period, p = lax.div(i, per_block), lax.rem(i, per_block)

        @pl.when(p <= trigger)
        def _():
            run(period, low, high, jnp.minimum(p * each, pieces), jnp.minimum((p + 1) * each, pieces))

        @pl.when(p == trigger)
        def _():
            stage(0, period, low, high)
            stage(1, period, low, high)
            if wait:
                stage(2, period - 1)

        if wait:
            @pl.when(i == span + trigger)
            def _():
                for r in range(pieces):
                    hidden[r] = jnp.square(jnp.maximum(acc[r], 0.0)).astype(jnp.bfloat16)

    def step(s, carry):
        forward(s)

        @pl.when(s >= LAG)
        def _():
            absorb(s - LAG, 0, 5, True)
        return carry

    lax.fori_loop(0, total, step, 0)
    def drain(low, high, wait, end):
        def one(i, carry):
            absorb(i, low, high, wait)
            return carry

        lax.fori_loop(total - LAG, end, one, 0)

    def finish(r, carry):
        m, k = lax.div(r, last), lax.rem(r, last)
        for way in range(2):
            @pl.when(has[way] & ((k == 0) | reach(way, k)))
            def _(way=way):
                all_rows(m, origin(way, k), way, k, False, half).wait_send()

            short = shortened(m, origin(way, k + 1), count - 1)
            for size, chosen in ((half, ~short), (half - extra, short)):
                @pl.when(reach(way, k + 1) & chosen)
                def _(way=way, size=size):
                    all_rows(m, origin(way, k + 1), way, k, True, size).wait_send()
        return carry

    def finish_all():
        lax.fori_loop(0, 2 * last, finish, 0)
        if extra:
            for way in range(2):
                @pl.when(has[way])
                def _(way=way):
                    extra_rows(way, ends[way]).wait_send()

    def take_extra():
        if extra:
            for way in range(2):
                @pl.when(f == ends[1 - way])
                def _(way=way):
                    extra_rows(way, ends[way]).wait_recv()

    def fill(which, index, low, high):
        for p in range(low, high):
            value = ending[which, p].astype(jnp.bfloat16)
            for j in range(tp):
                part[index, j, :, p * rows:(p + 1) * rows] = value[j * share:(j + 1) * share]

    def share_all(index):
        for j in range(1, tp):
            share_out(index, j).start()

    def collect(index):
        value = part[index, t].astype(jnp.float32)
        for j in range(1, tp):
            share_out(index, j).wait_recv()
            value = value + far[index, j - 1].astype(jnp.float32)
        out[index] = value.astype(jnp.bfloat16)

    drain(0, 2, False, total)
    if single:
        far_end = (f == 0) | (f == last)
        z_index = (last - f) * every + g * blocks + blocks - 1

        @pl.when(far_end)
        def _():
            fill(1, z_index, 0, per_block)
            share_all(z_index)

        drain(2, 5, True, total - 1)
        rest(total - 1, 2, 5, True)
        _, source, _ = x_of(total - 1)
        index = source * every + other * blocks + blocks - 1
        fill(0, index, 0, per_block - 1)
        take_extra()
        take(total - 1)
        ending[0, per_block - 1] = chunk_product(source, other, count - 1)
        fill(0, index, per_block - 1, per_block)
        share_all(index)
        finish_all()
        stage(2, final - 1)

        @pl.when(far_end)
        def _():
            collect(z_index)

        collect(index)
    else:
        take_extra()
        drain(2, 5, True, total)
        run(final, 0, 4, 0, pieces)
        stage(0, final, 0, 4)
        stage(1, final, 0, 4)
        finish_all()
        stage(2, final - 1)
        stage(2, final, 0, 4)
    for j in range(1, tp):
        pltpu.make_async_remote_copy(
            part.at[:, mate(j)], far.at[:, j - 1], ss.at[j - 1], sr.at[0],
            device_id=(g, f, mate(j)), device_id_type=MESH).wait_send()


def gather(n, tp, tokens, gain, up, down):
    local, width = up.shape
    count_rows = tokens.shape[0]
    half = local // 2
    block = divisor(half, 256, 16)
    rows = chunk_rows(block, width)
    count = half // rows
    depth = n * local
    piece = next(size for size in (512, 256, 128, width) if width % size == 0)
    moves = 2 * (n - 1) * count
    share, total = count_rows // tp, depth // block
    dma = pltpu.SemaphoreType.DMA
    step_rows = divisor(local, 128, 8)
    sent = 3 * (n - 1) * local * width * 2
    anywhere = pl.BlockSpec(memory_space=pl.ANY)
    inside = pl.BlockSpec(memory_space=pltpu.VMEM)
    return pl.pallas_call(
        functools.partial(gather_kernel, (n, tp, local, block, rows, piece)),
        out_shape=[
            pltpu.VMEM((2, depth, width), jnp.bfloat16),
            pltpu.VMEM((total, share, block), jnp.bfloat16),
        ],
        in_specs=[anywhere, inside, anywhere, anywhere],
        out_specs=[inside, inside],
        scratch_shapes=[
            pltpu.VMEM((min(SLOTS, 4 * count), rows, width), jnp.float32),
            pltpu.VMEM((local, 1), jnp.float32),
            pltpu.VMEM((count_rows, depth), jnp.bfloat16),
            pltpu.VMEM((depth // block, count_rows, block), jnp.bfloat16),
            pltpu.VMEM((width // piece, count_rows, piece), jnp.float32),
            pltpu.VMEM((width // piece, count_rows, piece), jnp.bfloat16),
            pltpu.VMEM((5, count_rows, block), jnp.float32),
            pltpu.VMEM((2, block // rows, count_rows, rows), jnp.float32),
            pltpu.VMEM((total, tp, share, block), jnp.bfloat16),
            pltpu.VMEM((total, tp - 1, share, block), jnp.bfloat16),
            dma((min(SLOTS, 4 * count),)),
            dma((1,)),
            dma((4 * (n - 1),)),
            dma((2 * moves,)),
            dma((4 * (n - 1),)),
            dma((moves,)),
            dma((2,)),
            dma((2,)),
            dma((tp - 1,)),
            dma((total * (tp - 1),)),
        ],
        compiler_params=pltpu.CompilerParams(
            collective_id=0, has_side_effects=True, vmem_limit_bytes=27 * 512 * 1024),
        cost_estimate=pl.CostEstimate(flops=0, bytes_accessed=sent, transcendentals=0),
        name="gather_both",
    )(tokens, gain.reshape(local // step_rows, step_rows), up, down)


def write_kernel(parts, both, mixed, up_ready, down_ready, mixed_out, done):
    depth = both.shape[1]
    size = depth // parts
    copies = []
    for m, ready in enumerate((up_ready, down_ready)):
        for i in range(parts):
            place = pl.ds(i * size, size)
            copies.append(pltpu.make_async_copy(both.at[m, place], ready.at[place], done.at[m * parts + i]))
    for copy in copies:
        copy.start()
    block = mixed.shape[2]
    for i in range(mixed.shape[0]):
        mixed_out[:, i * block:(i + 1) * block] = mixed[i]
    for copy in copies:
        copy.wait()


def per_device(n, tp, tokens, norm_gain, up_master, down_master):
    both, mixed = gather(n, tp, tokens, norm_gain, up_master, down_master)
    depth, width = both.shape[1:]
    share = mixed.shape[1]
    weight = jax.ShapeDtypeStruct((depth, width), jnp.bfloat16)
    anywhere = pl.BlockSpec(memory_space=pl.ANY)
    inside = pl.BlockSpec(memory_space=pltpu.VMEM)
    parts = 8
    return tuple(pl.pallas_call(
        functools.partial(write_kernel, parts),
        out_shape=[weight, weight, jax.ShapeDtypeStruct((share, depth), jnp.bfloat16)],
        in_specs=[anywhere, inside],
        out_specs=[anywhere, anywhere, inside],
        scratch_shapes=[pltpu.SemaphoreType.DMA((2 * parts,))],
        compiler_params=pltpu.CompilerParams(vmem_limit_bytes=27 * 512 * 1024),
        name="write_out",
    )(pltpu.with_memory_space_constraint(both, pltpu.VMEM), pltpu.with_memory_space_constraint(mixed, pltpu.VMEM)))


def solution(mesh):
    n, tp = (mesh.shape[name] for name in ("fs", "tp"))
    return jax.shard_map(
        functools.partial(per_device, n, tp),
        mesh=mesh,
        in_specs=(P(("grp", "fs"), None), P("fs"), P("fs", "tp"), P("fs", "tp")),
        out_specs=(P("grp", "tp"), P("grp", "tp"), P(("grp", "fs", "tp"), None)),
        check_vma=False,
    )
```
